512 devices in a mesh: ep: 32 (over z, x), tp: 16 (over y, core).
Axes of the slice: x: 4, y: 8, z: 8, core: 2. Of those that a mesh axis runs over, the one named last changes fastest.
Arguments:
- tokens: bfloat16 [4096, 2048], P('ep'), may hold values from -6 to 6
- routing: int32 [4096, 2], P('ep'), may hold values from 0 to 31, all different within a row; in each aligned block of 128 rows (0 to 127, 128 to 255, ...) at most 14 rows name the same one
- router_weight: bfloat16 [2048, 32], replicated, may hold values from -0.125 to 0.125
- gate_weight: bfloat16 [32, 2048, 2048], P('ep', None, 'tp'), may hold values from -0.125 to 0.125
- up_weight: bfloat16 [32, 2048, 2048], P('ep', None, 'tp'), may hold values from -0.125 to 0.125
- down_weight: bfloat16 [32, 2048, 2048], P('ep', 'tp'), may hold values from -0.125 to 0.125
- cotangent: bfloat16 [4096, 2048], P('ep'), may hold values from -0.796875 to 0.796875
Outputs:
- token_grad: bfloat16 [4096, 2048], P('ep')
- router_grad: float32 [2048, 32], P('tp')
- router_rows: float32 [2048], P('tp')
- gate_grad: bfloat16 [32, 2048, 2048], P('ep', None, 'tp')
- up_grad: bfloat16 [32, 2048, 2048], P('ep', None, 'tp')
- down_grad: bfloat16 [32, 2048, 2048], P('ep', 'tp')
- gate_rows: float32 [32, 2048], P('ep')
- up_rows: float32 [32, 2048], P('ep')
- down_rows: float32 [32, 2048], P('ep', 'tp')
The draws below stay inside these ranges and needn't reach their ends.
Inputs may be any that keep to these rules, and one draw needn't show every extreme that they name: `routing`: A row's 2 experts differ. Within the rows of one index of ep (128 rows), no expert is named more than 14 times, a bound that some block reaches.
All inputs are finite; a program needn't handle non-finite values.
Results may differ from the reference program's by a relative error of at most 0.01.
Values may be sent and summed in bfloat16 or wider, within the bound.
A program may use at most 64 MiB of HBM per device.

```python
import math
import jax
import jax.numpy as jnp
import numpy as np
from jax import lax

D = 2048
FF = 2048
TOPK = 2
TOK_DEV = 128
EXPERTS = 32
TOKENS = 4096
CAP = 14
N_EP = 32


def level_of(stream_key, shape, pieces, low, high):
    gain = 1.0
    for axis_at, parts in pieces:
        steps = jax.random.uniform(jax.random.fold_in(jax.random.fold_in(stream_key, 6), axis_at), (parts,), jnp.float32, low / len(pieces), high / len(pieces))
        gain = gain * jnp.repeat(jnp.exp(steps), shape[axis_at] // parts).reshape((-1,) + (1,) * (len(shape) - 1 - axis_at))
    return gain


def shared_out(rng, own, number, rows, number_of, top, most, lean):
    sequence = jax.random.permutation(rng, number_of)
    crowded, common = shares(number_of, rows * top, most, lean, True), shares(number_of, rows * top, most, lean, False)
    places = jnp.arange(number_of)

    def named(lengths, turn):
        used = int((lengths > 0).sum())
        fixed = max(1, used // 4)
        moved = fixed + (places - fixed + turn * (used - fixed)) % max(1, number_of - fixed)
        return jnp.zeros((number_of,), jnp.int32).at[sequence[jnp.where(places < fixed, places, moved)]].set(jnp.asarray(lengths, jnp.int32))

    lengths = jnp.where(number % 4 == 0, named(crowded, number // 4), named(common, number - number // 4 - 1))
    mixed = jax.random.permutation(jax.random.fold_in(own, 3), number_of)
    donor, sink = mixed[0:number_of // 2 * 2:2], mixed[1:number_of // 2 * 2:2]
    room = jnp.minimum(lengths[donor] - 1, most - lengths[sink]) // 2
    room = jnp.where((donor == sequence[0]) | (sink == sequence[0]) | (lengths[sink] == 0), 0, jnp.maximum(room, 0))
    moved = jax.random.randint(jax.random.fold_in(own, 4), (number_of // 2,), 0, 1 << 20) % (room + 1)
    lengths = lengths.at[donor].add(-moved).at[sink].add(moved)
    members = jnp.searchsorted(jnp.cumsum(lengths), jnp.arange(rows * top), side="right").astype(jnp.int32)
    grid = members.reshape(top, rows).T
    grid = grid[jax.random.permutation(jax.random.fold_in(own, 1), rows)]
    turn = jax.random.randint(jax.random.fold_in(own, 2), (rows, 1), 0, top)
    return jnp.take_along_axis(grid, (jnp.arange(top)[None, :] + turn) % top, axis=1)


def shares(number_of, total, bound, lean, full):
    portions = [(1 << 20) // math.isqrt(standing ** lean) + 1 for standing in range(1, number_of + 1)]
    largest = bound if full else min(bound, max(-(-total // number_of), total * portions[0] // sum(portions)))
    least = 1 if total - largest >= number_of - 1 else 0
    holding, spare = [largest] + [least] * (number_of - 1), total - largest - least * (number_of - 1)
    while spare > 0:
        candidates = [i for i in range(1, number_of) if holding[i] < largest] or [i for i in range(1, number_of) if holding[i] < bound]
        whole, left = sum([portions[i] for i in candidates]), spare
        for i in candidates:
            extra = min(bound - holding[i], max(1, left * portions[i] // whole), spare)
            holding[i] = holding[i] + extra
            spare = spare - extra
    return np.array(holding)


def gaussian(stream_key, extent, width, reach, split=(), held_as=jnp.bfloat16):
    drawn = width * jax.random.normal(stream_key, extent, jnp.float32)
    if split:
        drawn = drawn * level_of(stream_key, extent, split, -0.22, 0.18)
    return jnp.clip(drawn, -reach, reach).astype(held_as)


def setup_inputs(seed: int = 0) -> dict:
    keys = jax.random.split(jax.random.key(seed), 8)
    tokens = gaussian(keys[0], (TOKENS, D), 1.0, 6.0, ((0, 32),))
    routing_keys = jax.random.split(jax.random.fold_in(keys[1], 1), TOKENS // TOK_DEV)
    routing_turns = jax.random.permutation(jax.random.fold_in(keys[1], 3), TOKENS // TOK_DEV)
    routing = jax.vmap(lambda own, number: shared_out(jax.random.fold_in(keys[1], 2), own, number, TOK_DEV, EXPERTS, TOPK, CAP, 2))(routing_keys, routing_turns).reshape((TOKENS, TOPK))
    router_weight = gaussian(keys[2], (D, EXPERTS), D ** -0.5, 0.125)
    gate_weight = gaussian(keys[3], (EXPERTS, D, FF), D ** -0.5, 0.125, ((0, 32), (2, 16)))
    up_weight = gaussian(keys[4], (EXPERTS, D, FF), D ** -0.5, 0.125, ((0, 32), (2, 16)))
    down_weight = gaussian(keys[5], (EXPERTS, FF, D), FF ** -0.5, 0.125, ((0, 32), (1, 16)))
    cotangent = gaussian(keys[6], (TOKENS, D), 0.1, 0.796875, ((0, 32),))
    return dict(tokens=tokens, routing=routing, router_weight=router_weight, gate_weight=gate_weight, up_weight=up_weight, down_weight=down_weight, cotangent=cotangent)


def block_slots(route_block):
    flat_ids = route_block.reshape(-1)
    onehot = (flat_ids[:, None] == jnp.arange(EXPERTS, dtype=jnp.int32)[None, :]).astype(jnp.int32)
    position = jnp.sum((jnp.cumsum(onehot, axis=0) - 1) * onehot, axis=1)
    return flat_ids, position.astype(jnp.int32)


def expert_backward(rows_in, cots_in, slot_scale, w_gate, w_up, w_down):
    pre_gate = jnp.dot(rows_in, w_gate, preferred_element_type=jnp.float32)
    pre_up = jnp.dot(rows_in, w_up, preferred_element_type=jnp.float32)
    sigmoid_gate = jax.nn.sigmoid(pre_gate)
    hidden = (pre_gate * sigmoid_gate * pre_up).astype(jnp.bfloat16)
    back_proj = lax.dot_general(cots_in, w_down, (((1,), (1,)), ((), ())), preferred_element_type=jnp.float32)
    gate_term = jnp.sum(hidden.astype(jnp.float32) * back_proj, axis=1)
    scaled = slot_scale * back_proj
    grad_up_pre = (scaled * pre_gate * sigmoid_gate).astype(jnp.bfloat16)
    grad_gate_pre = (scaled * pre_up * sigmoid_gate * (1.0 + pre_gate * (1.0 - sigmoid_gate))).astype(jnp.bfloat16)
    weighted = (slot_scale * cots_in.astype(jnp.float32)).astype(jnp.bfloat16)
    contract_rows = (((0,), (0,)), ((), ()))
    grad_down = lax.dot_general(hidden, weighted, contract_rows, preferred_element_type=jnp.float32)
    grad_gate = lax.dot_general(rows_in, grad_gate_pre, contract_rows, preferred_element_type=jnp.float32)
    grad_up = lax.dot_general(rows_in, grad_up_pre, contract_rows, preferred_element_type=jnp.float32)
    contract_hidden = (((1,), (1,)), ((), ()))
    partial_value = lax.dot_general(grad_gate_pre, w_gate, contract_hidden, preferred_element_type=jnp.float32)
    partial_value = partial_value + lax.dot_general(grad_up_pre, w_up, contract_hidden, preferred_element_type=jnp.float32)
    return partial_value, gate_term, grad_gate, grad_up, grad_down


def reference(tokens, routing, router_weight, gate_weight, up_weight, down_weight, cotangent):
    logits = jnp.dot(tokens, router_weight, preferred_element_type=jnp.float32)
    affinity = jax.nn.sigmoid(logits)
    chosen = jnp.take_along_axis(affinity, routing, axis=1)
    total_aff = jnp.sum(chosen, axis=1, keepdims=True)
    weights = chosen / total_aff
    assigns = TOKENS * TOPK
    flat_ids, positions = jax.vmap(block_slots)(routing.reshape(N_EP, TOK_DEV, TOPK))
    source = jnp.arange(N_EP, dtype=jnp.int32)[:, None]
    slot_index = ((flat_ids * N_EP + source) * CAP + positions).reshape(-1)
    slot_table = jnp.full((EXPERTS * N_EP * CAP,), assigns, jnp.int32)
    slot_table = slot_table.at[slot_index].set(jnp.arange(assigns, dtype=jnp.int32))
    slot_table = slot_table.reshape(EXPERTS, N_EP * CAP)
    zero_row = jnp.zeros((1, D), jnp.bfloat16)
    tok_pad = jnp.concatenate([tokens, zero_row], axis=0)
    cot_pad = jnp.concatenate([cotangent, zero_row], axis=0)
    weight_pad = jnp.concatenate([weights.astype(jnp.bfloat16).reshape(-1), jnp.zeros((1,), jnp.bfloat16)])

    def expert(operands):
        slot_ids, w_gate, w_up, w_down = operands
        rows_in = tok_pad[slot_ids // TOPK]
        cots_in = cot_pad[slot_ids // TOPK]
        slot_scale = weight_pad[slot_ids].astype(jnp.float32)[:, None]
        return expert_backward(rows_in, cots_in, slot_scale, w_gate, w_up, w_down)

    partial_value, gate_term, grad_gate, grad_up, grad_down = lax.map(expert, (slot_table, gate_weight, up_weight, down_weight))
    gate_rows = jnp.sum(grad_gate * grad_gate, axis=2)
    up_rows = jnp.sum(grad_up * grad_up, axis=2)
    down_rows = jnp.sum(grad_down * grad_down, axis=2)
    flat_table = slot_table.reshape(-1)
    slot_grad = jnp.zeros((assigns + 1, D), jnp.bfloat16).at[flat_table].set(partial_value.astype(jnp.bfloat16).reshape(-1, D))
    slot_gate = jnp.zeros((assigns + 1,), jnp.bfloat16).at[flat_table].set(gate_term.astype(jnp.bfloat16).reshape(-1))
    back_rows = jnp.sum(slot_grad[:assigns].astype(jnp.float32).reshape(TOKENS, TOPK, D), axis=1)
    d_weights = slot_gate[:assigns].astype(jnp.float32).reshape(TOKENS, TOPK)
    d_chosen = (d_weights - jnp.sum(d_weights * weights, axis=1, keepdims=True)) / total_aff
    d_logit = d_chosen * chosen * (1.0 - chosen)
    onehot = (routing[:, :, None] == jnp.arange(EXPERTS, dtype=jnp.int32)[None, None, :]).astype(jnp.float32)
    d_logits = jnp.sum(d_logit[:, :, None] * onehot, axis=1).astype(jnp.bfloat16)
    router_grad = lax.dot_general(tokens, d_logits, (((0,), (0,)), ((), ())), preferred_element_type=jnp.float32)
    router_rows = jnp.sum(router_grad * router_grad, axis=1)
    router_back = lax.dot_general(d_logits, router_weight, (((1,), (1,)), ((), ())), preferred_element_type=jnp.float32)
    token_grad = (back_rows + router_back).astype(jnp.bfloat16)
    return (token_grad, router_grad, router_rows, grad_gate.astype(jnp.bfloat16), grad_up.astype(jnp.bfloat16),
            grad_down.astype(jnp.bfloat16), gate_rows, up_rows, down_rows)
```

```python
import functools

import jax
import jax.numpy as jnp
from jax import lax
from jax.experimental import pallas as pl
from jax.experimental.pallas import tpu as pltpu
from jax.sharding import PartitionSpec as P

BF = jnp.bfloat16
F32 = jnp.float32
CW = 128
SUB = 112
HI = lax.Precision.HIGHEST
NN = ((1,), (0,))
NT = ((1,), (1,))
TN = ((0,), (0,))


def dot(a, b, dims=NN, precision=None):
    return lax.dot_general(a, b, (dims, ((), ())), precision=precision, preferred_element_type=F32)


def iota(shape, dim):
    return lax.broadcasted_iota(jnp.int32, shape, dim)


def one_hot(mask, dtype=BF):
    return jnp.where(mask, 1.0, 0.0).astype(dtype)


def kernel(
    cfg,
    routing, rw, tok_h, cot_h, gw_h, uw_h, dw_h,
    tg_o, rg_o, rr_o, gg_o, ug_o, dg_o, rows_o, drow_o,
    tok_v, cot_v, w_own, w_par, dn_v,
    sel_v, cmp_v, sx, rx, sz, rz_, xa, za, wcol, acc_gu, acc_b,
    hid_v, gp_own, gp_par, tm_v, part_v, rs_s, rs_r, ret_s, ret_r,
    g_s, g_r, gf_r, zr_r, xr_s, xr_r, row_v, rowd_r, rowy_s, rowy_r, rowf_s, tg_r,
    ld_sem, a_send, a_recv, y_send, y_recv, d_send, d_recv, w_send, w_recv, gp_send, gp_recv,
    g_send, g_recv, gf_send, gf_recv, rs_send, rs_recv, ret_send, ret_recv,
    z_send, z_recv, x_send, x_recv, rd_send, rd_recv, ry_send, ry_recv, rf_send, rf_recv,
    t_send, t_recv, td_send, td_recv,
):
    EP, NX, NY, T, D, CAP, PC = cfg
    NZ = EP // NX
    TP = 2 * NY
    H = NY // 2
    ROWS = EP * CAP
    SLOTS = EP * PC
    NS = ROWS // SUB
    shift = PC.bit_length() - 1
    inv = 65536 // CAP + 1
    ep = lax.axis_index("ep")
    tp = lax.axis_index("tp")
    y = lax.div(tp, 2)
    c = lax.rem(tp, 2)
    zc = lax.div(ep, NX)
    xc = lax.rem(ep, NX)
    partner = {"tp": y * 2 + (1 - c)}

    def ydev(off):
        return {"tp": lax.rem(y + off + NY, NY) * 2 + c}

    def remote(src, dst, ss, rs, dev):
        return pltpu.make_async_remote_copy(
            src_ref=src, dst_ref=dst, send_sem=ss, recv_sem=rs, device_id=dev,
            device_id_type=pl.DeviceIdType.MESH,
        )

    def each(lo, hi, body):
        def step(i, carry):
            body(i)
            return carry

        lax.fori_loop(lo, hi, step, 0)

    cols = pl.ds(pl.multiple_of(tp * CW, CW), CW)
    ld_tok = pltpu.make_async_copy(tok_h, tok_v, ld_sem.at[0])
    ld_cot = pltpu.make_async_copy(cot_h.at[:, cols], cot_v, ld_sem.at[1])
    ld_g = pltpu.make_async_copy(gw_h.at[0], w_own.at[0], ld_sem.at[2])
    ld_u = pltpu.make_async_copy(uw_h.at[0], w_own.at[1], ld_sem.at[3])
    ld_d = pltpu.make_async_copy(dw_h.at[0], dn_v, ld_sem.at[4])
    for cp in (ld_tok, ld_cot, ld_g, ld_u, ld_d):
        cp.start()
    barrier = pltpu.get_barrier_semaphore()

    def greet_ep(d):
        pl.semaphore_signal(barrier, inc=1, device_id={"ep": lax.rem(ep + d, EP)},
                            device_id_type=pl.DeviceIdType.MESH)

    def greet_tp(d):
        pl.semaphore_signal(barrier, inc=1, device_id={"tp": lax.rem(tp + d, TP)},
                            device_id_type=pl.DeviceIdType.MESH)

    each(1, EP, greet_ep)
    each(1, TP, greet_tp)

    e_lane = iota((T, EP), 1)
    chosen_mask = (e_lane == routing[:, 0:1]) | (e_lane == routing[:, 1:2])
    hit = one_hot(chosen_mask)
    earlier = one_hot(iota((T, T), 1) < iota((T, T), 0))
    count = dot(earlier, hit).astype(BF)
    spread = one_hot((iota((EP, SLOTS), 1) >> shift) == iota((EP, SLOTS), 0))
    slot_lane = (iota((T, SLOTS), 1) & (PC - 1)).astype(F32)
    sel = jnp.where((dot(count, spread) == slot_lane) & (dot(hit, spread) > 0.5), 1.0, 0.0)
    sel_v[...] = sel.astype(BF)
    lane_of = one_hot((iota((SLOTS, CW), 0) & (PC - 1)) == iota((SLOTS, CW), 1))
    tail = one_hot(
        ((iota((SLOTS, EP), 0) >> shift) == iota((SLOTS, EP), 1))
        & ((iota((SLOTS, EP), 0) & (PC - 1)) == CAP)
    )
    row_id = iota((ROWS, SLOTS), 0)
    row_src = (row_id * inv) >> 16
    cmp_v[...] = one_hot(iota((ROWS, SLOTS), 1) == row_id + (PC - CAP) * row_src)

    ld_tok.wait()
    affinity = jax.nn.sigmoid(dot(tok_v[...], rw[...]))
    hit32 = hit.astype(F32)
    chosen = affinity * hit32
    total = jnp.sum(chosen, axis=1, keepdims=True)
    weights = chosen / total
    wx = dot(weights.astype(BF), spread)
    slot_w = jnp.sum(sel * wx, axis=0, keepdims=True)
    w_rows = dot((spread.astype(F32) * slot_w).astype(BF), lane_of)
    tok_cols = tok_v[:, cols]
    ld_cot.wait()
    send_x = dot(sel.astype(BF), tok_cols, TN) + dot(tail, w_rows.astype(BF))
    sx[...] = send_x.astype(BF).reshape(EP, PC, CW)
    sz[...] = dot(sel.astype(BF), cot_v[...], TN).astype(BF).reshape(EP, PC, CW)

    pl.semaphore_wait(barrier, EP - 1 + TP - 1)

    def a2a(part, src, dst, peer):
        return remote(src.at[peer], dst.at[ep], a_send.at[part, peer], a_recv.at[part, ep], {"ep": peer})

    def a2a_wait(part, src, dst, peer):
        return remote(src.at[peer], dst.at[peer], a_send.at[part, peer], a_recv.at[part, peer], {"ep": peer})

    def peer_of(d):
        return lax.rem(ep + d, EP)

    each(1, EP, lambda d: a2a(0, sx, rx, peer_of(d)).start())
    each(1, EP, lambda d: a2a(1, sz, rz_, peer_of(d)).start())
    rx[ep] = sx[ep]
    rz_[ep] = sz[ep]
    ld_g.wait()
    ld_u.wait()
    ld_d.wait()
    cp_w = remote(w_own, w_par, w_send, w_recv, partner)
    cp_w.start()

    bufs = (xa, za)

    def hop(way, step, part, src):
        blk = bufs[part].at[src, c]
        return remote(blk, blk, y_send.at[way, step - 1, part], y_recv.at[way, step - 1, part],
                      ydev(1 if way == 0 else -1))

    def cross(part, src):
        blk = bufs[part].at[src, c]
        return remote(blk, blk, d_send.at[part, src], d_recv.at[part, src], partner)

    def cross_wait(part, src):
        blk = bufs[part].at[src, 1 - c]
        remote(blk, blk, d_send.at[part, src], d_recv.at[part, src], partner).wait_recv()

    each(1, EP, lambda d: a2a_wait(0, sx, rx, peer_of(d)).wait_recv())
    rx_all = rx[...].reshape(SLOTS, CW)
    xa[y, c] = dot(cmp_v[...], rx_all).astype(BF)
    hop(0, 1, 0, y).start()
    if H > 1:
        hop(1, 1, 0, y).start()
    cross(0, y).start()
    each(1, EP, lambda d: a2a_wait(1, sz, rz_, peer_of(d)).wait_recv())
    za[y, c] = dot(cmp_v[...], rz_[...].reshape(SLOTS, CW)).astype(BF)
    if H > 1:
        hop(0, 1, 1, y).start()
    hop(1, 1, 1, y).start()
    cross(1, y).start()

    pick = one_hot(
        iota((ROWS, SLOTS), 1) == (row_src * PC + CAP)
    )
    w_sel = dot(pick, rx_all)
    r2 = iota((ROWS, CW), 0)
    r2_pos = r2 - ((r2 * inv) >> 16) * CAP
    w_masked = jnp.where(r2_pos == iota((ROWS, CW), 1), w_sel, 0.0)
    wcol[...] = jnp.broadcast_to(jnp.sum(w_masked, axis=1, keepdims=True), (ROWS, CW))

    acc_gu[...] = jnp.zeros_like(acc_gu)
    acc_b[...] = jnp.zeros_like(acc_b)

    def chunk_ds(src):
        return pl.ds(pl.multiple_of(src * 2 * CW, 2 * CW), 2 * CW)

    def forward_chunk(src):
        cross_wait(0, src)
        xs = jnp.concatenate([xa[src, 0], xa[src, 1]], axis=1)
        ds = chunk_ds(src)
        wgu = jnp.concatenate([w_own[0, ds, :], w_own[1, ds, :]], axis=1)
        acc_gu[...] += dot(xs, wgu)
        cross_wait(1, src)
        zs = jnp.concatenate([za[src, 0], za[src, 1]], axis=1)
        acc_b[...] += dot(zs, dn_v[:, ds], NT)

    def at(off):
        return lax.rem(y + off + NY, NY)

    def parts_of(way, step):
        return (0, 1) if step < H else ((0,) if way == 0 else (1,))

    each(0, 1, lambda i: forward_chunk(at(i)))
    for s in range(1, H + 1):
        for part in (0, 1):
            for way in (0, 1):
                if part not in parts_of(way, s):
                    continue
                src = at(-s if way == 0 else s)
                hop(way, s, part, src).wait_recv()
                if s < H and part in parts_of(way, s + 1):
                    hop(way, s + 1, part, src).start()
                cross(part, src).start()
        if s < H:
            each(0, 2, lambda i, s=s: forward_chunk(at((2 * i - 1) * s)))
    each(0, 1, lambda i: forward_chunk(at(H + i)))

    RB = 32

    def pointwise(i):
        ds = pl.ds(pl.multiple_of(i * RB, RB), RB)
        pg = acc_gu[ds, :CW]
        pu = acc_gu[ds, CW:]
        bk = acc_b[ds, :]
        s = jax.nn.sigmoid(pg)
        hid = (pg * s * pu).astype(BF)
        hid_v[ds, :] = hid
        term = jnp.sum(hid.astype(F32) * bk, axis=1, keepdims=True)
        rr = iota((RB, CW), 0) + i * RB
        pos = rr - ((rr * inv) >> 16) * CAP
        tm_v[ds, :] = jnp.where(pos == iota((RB, CW), 1), term, 0.0)
        sc = wcol[ds, :] * bk
        gp_own[ds, :CW] = (sc * pu * s * (1.0 + pg * (1.0 - s))).astype(BF)
        gp_own[ds, CW:] = (sc * pg * s).astype(BF)

    each(0, ROWS // RB, pointwise)
    cp_gp = remote(gp_own, gp_par, gp_send, gp_recv, partner)
    cp_gp.start()

    block_of = one_hot(((iota((EP, ROWS), 1) * inv) >> 16) == iota((EP, ROWS), 0), F32)
    g_s[...] = dot(block_of, tm_v[...], NN, HI).reshape(EP, 1, CW)
    g_r[ep] = g_s[ep]

    def g_copy(peer, slot):
        return remote(g_s.at[peer], g_r.at[slot], g_send.at[peer], g_recv.at[slot], {"ep": peer})

    each(1, EP, lambda d: g_copy(peer_of(d), ep).start())

    cp_w.wait_recv()
    cp_gp.wait_recv()

    def partial_for(off):
        base = pl.multiple_of(at(off) * 2 * CW + c * CW, CW)
        ds = pl.ds(base, CW)
        own = jnp.concatenate([w_own[0, ds, :], w_own[1, ds, :]], axis=1)
        par = jnp.concatenate([w_par[0, ds, :], w_par[1, ds, :]], axis=1)
        return dot(gp_own[...], own, NT) + dot(gp_par[...], par, NT)

    def rs(way, step, i):
        ds = pl.ds(i * SUB, SUB)
        return remote(rs_s.at[way, step - 1, ds], rs_r.at[way, step - 1, ds],
                      rs_send.at[way, step - 1, i], rs_recv.at[way, step - 1, i],
                      ydev(1 if way == 0 else -1))

    def subs(way, step):
        if step > 1:
            return tuple(range(NS))
        return tuple(range(NS // 2, NS)) if way == 0 else tuple(range(NS // 2))

    first = partial_for(H)
    for way in (0, 1):
        half = pl.ds(subs(way, 1)[0] * SUB, ROWS // 2)
        lo = subs(way, 1)[0] * SUB
        rs_s[way, 0, half] = first[lo:lo + ROWS // 2].astype(BF)
        for i in subs(way, 1):
            rs(way, 1, i).start()

    def own_parts(step):
        part_v[0] = partial_for(H - step + 1)
        part_v[1] = partial_for(-(H - step + 1))

    def rs_step(step):
        have = [(i, w) for i in range(NS) for w in (0, 1)]
        have.sort(key=lambda t: (t[0] in subs(t[1], step - 1)))
        for i, w in have:
            ds = pl.ds(i * SUB, SUB)
            val = part_v[w, ds, :]
            if i in subs(w, step - 1):
                rs(w, step - 1, i).wait_recv()
                val = val + rs_r[w, step - 2, ds, :].astype(F32)
            rs_s[w, step - 1, ds, :] = val.astype(BF)
            rs(w, step, i).start()

    ones = jnp.ones((8, 2 * CW), BF)
    drow_o[...] = jnp.zeros_like(drow_o)

    def grads(src):
        ds = chunk_ds(src)
        xs = jnp.concatenate([xa[src, 0], xa[src, 1]], axis=1)
        gu = dot(xs, gp_own[...], TN)
        gg_o[ds, :] = gu[:, :CW].astype(BF)
        ug_o[ds, :] = gu[:, CW:].astype(BF)
        sq = (gu * gu).astype(BF)
        for k in (0, 1):
            tot = dot(ones[:, :CW], sq[:, k * CW:(k + 1) * CW], NT)
            row_v[k, pl.ds(src * 2, 1)] = tot[0:1, :CW].reshape(1, 1, CW)
            row_v[k, pl.ds(src * 2 + 1, 1)] = tot[0:1, CW:].reshape(1, 1, CW)
        scale = wcol[...]
        w0 = (scale * za[src, 0].astype(F32)).astype(BF)
        w1 = (scale * za[src, 1].astype(F32)).astype(BF)
        dgr = dot(hid_v[...], jnp.concatenate([w0, w1], axis=1), TN)
        dg_o[:, ds] = dgr.astype(BF)
        drow_o[...] += dot(ones, (dgr * dgr).astype(BF), NT)

    per = -(-NY // H)

    def some_grads(k):
        each(k * per, min(NY, (k + 1) * per), grads)

    own_parts(2)
    some_grads(0)
    rs_step(2)

    each(1, EP, lambda d: g_copy(peer_of(d), peer_of(d)).wait_recv())
    lane_t = one_hot((iota((CW, SLOTS), 1) & (PC - 1)) == iota((CW, SLOTS), 0), F32)
    spread32 = one_hot((iota((EP, SLOTS), 1) >> shift) == iota((EP, SLOTS), 0), F32)
    g_flat = jnp.sum(dot(g_r[...].reshape(EP, CW), lane_t, NN, HI) * spread32, axis=0, keepdims=True)
    gf_r[tp] = g_flat

    def gf(peer, slot):
        return remote(gf_r.at[tp], gf_r.at[slot], gf_send.at[peer], gf_recv.at[slot], {"tp": peer})

    def gf_wait(peer):
        remote(gf_r.at[peer], gf_r.at[peer], gf_send.at[peer], gf_recv.at[peer], {"tp": peer}).wait_recv()

    def tpeer(d):
        return lax.rem(tp + d, TP)

    each(1, TP, lambda d: gf(tpeer(d), tp).start())

    def rs_rest(step):
        own_parts(step)
        some_grads(step - 2)
        rs_step(step)

    for step in range(3, H + 1):
        rs_rest(step)
        if step == 3:
            gather_terms = True
    each(1, TP, lambda d: gf_wait(tpeer(d)))
    g_tot = gf_r[0]
    for j in range(1, TP):
        g_tot = g_tot + gf_r[j]
    g_tot = g_tot.astype(BF).astype(F32)
    d_w = dot((sel_v[...].astype(F32) * g_tot).astype(BF), one_hot(
        (iota((SLOTS, EP), 0) >> shift) == iota((SLOTS, EP), 1)))
    d_chosen = (d_w - jnp.sum(d_w * weights, axis=1, keepdims=True)) / total
    d_logits = (d_chosen * chosen * (1.0 - affinity) * hit32).astype(BF)
    tok_c = tok_v[:, cols]
    zr_r[zc] = dot(d_logits, tok_c, TN)

    def zdev(off):
        return {"ep": lax.rem(zc + off, NZ) * NX + xc}

    def zsend(d):
        return remote(zr_r.at[zc], zr_r.at[zc], z_send.at[d - 1], z_recv.at[zc], zdev(d))

    def zwait(d):
        k = lax.rem(zc + d, NZ)
        remote(zr_r.at[k], zr_r.at[k], z_send.at[d - 1], z_recv.at[k], zdev(d)).wait_recv()

    each(1, NZ, lambda d: zsend(d).start())

    some_grads(H - 1)
    own = partial_for(0)

    hb = D // CW

    def rowd(k):
        return remote(row_v.at[k], rowd_r, rd_send, rd_recv, partner)

    rowd(1 - c).start()

    rd_wait = rowd(1 - c)

    out_rows = []
    for i in range(NS):
        ds = pl.ds(i * SUB, SUB)
        val = own[i * SUB:(i + 1) * SUB]
        for w in (0, 1):
            rs(w, H, i).wait_recv()
            val = val + rs_r[w, H - 1, ds, :].astype(F32)
        out_rows.append(val.astype(BF))
    slot_grad = jnp.concatenate(out_rows, axis=0)
    ret_s[...] = dot(cmp_v[...], slot_grad, TN).astype(BF).reshape(EP, PC, CW)

    def ret(peer, slot):
        return remote(ret_s.at[peer], ret_r.at[slot], ret_send.at[peer], ret_recv.at[slot], {"ep": peer})

    each(1, EP, lambda d: ret(peer_of(d), ep).start())
    ret_r[ep] = ret_s[ep]

    rd_wait.wait_recv()
    rowy_r[y] = row_v[c] + rowd_r[...]

    def ry(d):
        return remote(rowy_r.at[y], rowy_r.at[y], ry_send.at[d - 1], ry_recv.at[y], ydev(d))

    def ry_wait(d):
        k = at(d)
        remote(rowy_r.at[k], rowy_r.at[k], ry_send.at[d - 1], ry_recv.at[k], ydev(d)).wait_recv()

    each(1, NY, lambda d: ry(d).start())

    each(1, NZ, lambda d: zwait(d))
    z_tot = zr_r[0]
    for j in range(1, NZ):
        z_tot = z_tot + zr_r[j]
    xr_r[xc] = z_tot

    def xdev(off):
        return {"ep": zc * NX + lax.rem(xc + off, NX)}

    def xsend(d):
        return remote(xr_r.at[xc], xr_r.at[xc], x_send.at[d - 1], x_recv.at[xc], xdev(d))

    def xwait(d):
        k = lax.rem(xc + d, NX)
        remote(xr_r.at[k], xr_r.at[k], x_send.at[d - 1], x_recv.at[k], xdev(d)).wait_recv()

    each(1, NX, lambda d: xsend(d).start())
    router_back = dot(d_logits, rw[cols, :], NT)

    each(1, EP, lambda d: ret(peer_of(d), peer_of(d)).wait_recv())
    back = dot(sel_v[...], ret_r[...].reshape(SLOTS, CW))
    tg_r[y, c] = (back + router_back).astype(BF)

    def tg(d):
        blk = tg_r.at[y, c]
        return remote(blk, blk, t_send.at[d - 1], t_recv.at[y], ydev(d))

    def tg_wait(d):
        blk = tg_r.at[at(d), c]
        remote(blk, blk, t_send.at[d - 1], t_recv.at[at(d)], ydev(d)).wait_recv()

    def tgd(src):
        blk = tg_r.at[src, c]
        return remote(blk, blk, td_send.at[src], td_recv.at[src], partner)

    def tgd_wait(src):
        blk = tg_r.at[src, 1 - c]
        remote(blk, blk, td_send.at[src], td_recv.at[src], partner).wait_recv()

    each(1, NY, lambda d: tg(d).start())
    tgd(y).start()

    each(1, NY, lambda d: ry_wait(d))
    r_tot = rowy_r[0]
    for j in range(1, NY):
        r_tot = r_tot + rowy_r[j]
    rowf_s[c] = r_tot
    rf = remote(rowf_s.at[c], rowf_s.at[c], rf_send, rf_recv, partner)
    rf.start()
    each(1, NX, lambda d: xwait(d))
    x_tot = xr_r[0]
    for j in range(1, NX):
        x_tot = x_tot + xr_r[j]
    rg_o[...] = x_tot
    rr_o[...] = jnp.sum(x_tot * x_tot, axis=0, keepdims=True)

    def arrive(d):
        tg_wait(d)
        tgd(at(d)).start()

    each(1, NY, arrive)
    remote(rowf_s.at[1 - c], rowf_s.at[1 - c], rf_send, rf_recv, partner).wait_recv()
    rows_o[...] = rowf_s[...]
    each(0, NY, tgd_wait)
    for j in range(NY):
        for k in (0, 1):
            tg_o[:, (2 * j + k) * CW:(2 * j + k + 1) * CW] = tg_r[j, k]

    def drain_ep(d):
        p = peer_of(d)
        a2a(0, sx, rx, p).wait_send()
        a2a(1, sz, rz_, p).wait_send()
        g_copy(p, ep).wait_send()
        ret(p, ep).wait_send()

    each(1, EP, drain_ep)
    each(1, TP, lambda d: gf(tpeer(d), tp).wait_send())
    each(1, NZ, lambda d: zsend(d).wait_send())
    each(1, NX, lambda d: xsend(d).wait_send())

    def drain_y(d):
        ry(d).wait_send()
        tg(d).wait_send()

    each(1, NY, drain_y)

    def drain_d(s):
        cross(0, s).wait_send()
        cross(1, s).wait_send()
        tgd(s).wait_send()

    each(0, NY, drain_d)
    for s in range(1, H + 1):
        for way in (0, 1):
            for part in parts_of(way, s):
                hop(way, s, part, y).wait_send()
            for i in subs(way, s):
                rs(way, s, i).wait_send()
    cp_w.wait_send()
    cp_gp.wait_send()
    rd_wait.wait_send()
    rf.wait_send()


def build(ep, nx, ny, tok, width, cap):
    pc = 1
    while pc <= cap:
        pc *= 2
    rows, slots, tp, half = ep * cap, ep * pc, 2 * ny, ny // 2
    ns = rows // SUB
    hb = width // CW
    nz = ep // nx
    cfg = (ep, nx, ny, tok, width, cap, pc)
    v = pltpu.VMEM
    dma = pltpu.SemaphoreType.DMA
    scratch = [
        v((tok, width), BF), v((tok, CW), BF), v((2, width, CW), BF), v((2, width, CW), BF), v((CW, width), BF),
        v((tok, slots), BF), v((rows, slots), BF),
        v((ep, pc, CW), BF), v((ep, pc, CW), BF), v((ep, pc, CW), BF), v((ep, pc, CW), BF),
        v((ny, 2, rows, CW), BF), v((ny, 2, rows, CW), BF),
        v((rows, CW), F32), v((rows, 2 * CW), F32), v((rows, CW), F32),
        v((rows, CW), BF), v((rows, 2 * CW), BF), v((rows, 2 * CW), BF), v((rows, CW), F32),
        v((2, rows, CW), F32), v((2, half, rows, CW), BF), v((2, half, rows, CW), BF),
        v((ep, pc, CW), BF), v((ep, pc, CW), BF),
        v((ep, 1, CW), F32), v((ep, 1, CW), F32), v((tp, 1, slots), F32),
        v((nz, ep, CW), F32), v((ep, CW), F32), v((nx, ep, CW), F32),
        v((2, hb, 1, CW), F32), v((hb, 1, CW), F32), v((hb, 1, CW), F32), v((ny, hb, 1, CW), F32),
        v((2, hb, 1, CW), F32), v((ny, 2, tok, CW), BF),
        dma((5,)), dma((2, ep)), dma((2, ep)), dma((2, half, 2)), dma((2, half, 2)),
        dma((2, ny)), dma((2, ny)), dma, dma, dma, dma,
        dma((ep,)), dma((ep,)), dma((tp,)), dma((tp,)), dma((2, half, ns)), dma((2, half, ns)),
        dma((ep,)), dma((ep,)), dma((nz,)), dma((nz,)), dma((nx,)), dma((nx,)), dma, dma,
        dma((ny,)), dma((ny,)), dma, dma, dma((ny,)), dma((ny,)), dma((ny,)), dma((ny,)),
    ]
    out_shape = (
        jax.ShapeDtypeStruct((tok, width), BF),
        jax.ShapeDtypeStruct((ep, CW), F32),
        jax.ShapeDtypeStruct((1, CW), F32),
        jax.ShapeDtypeStruct((width, CW), BF),
        jax.ShapeDtypeStruct((width, CW), BF),
        jax.ShapeDtypeStruct((CW, width), BF),
        jax.ShapeDtypeStruct((2, hb, 1, CW), F32),
        jax.ShapeDtypeStruct((8, CW), F32),
    )
    vm = pl.BlockSpec(memory_space=pltpu.VMEM)
    hb_ = pl.BlockSpec(memory_space=pl.ANY)
    call = pl.pallas_call(
        functools.partial(kernel, cfg),
        out_shape=out_shape,
        in_specs=[vm, vm, hb_, hb_, hb_, hb_, hb_],
        out_specs=tuple([vm] * 8),
        scratch_shapes=scratch,
        compiler_params=pltpu.CompilerParams(
            collective_id=0, has_side_effects=True, vmem_limit_bytes=56 * 1024 * 1024
        ),
        name="experts_backward",
    )

    def per_device(tokens, routing, router_weight, gate_weight, up_weight, down_weight, cotangent):
        tg, rg, rr, gg, ug, dg, rows2, drow = call(
            routing, router_weight, tokens, cotangent, gate_weight, up_weight, down_weight
        )
        return (
            tg, rg.T, rr.reshape(CW), gg[None], ug[None], dg[None],
            rows2[0].reshape(1, width), rows2[1].reshape(1, width), drow[0:1],
        )

    return per_device


SPECS_IN = (
    P("ep", None), P("ep", None), P(), P("ep", None, "tp"), P("ep", None, "tp"), P("ep", "tp", None), P("ep", None),
)
SPECS_OUT = (
    P("ep", None), P("tp", None), P("tp"), P("ep", None, "tp"), P("ep", None, "tp"), P("ep", "tp", None),
    P("ep", None), P("ep", None), P("ep", "tp"),
)


def solution(mesh):
    ep, tp = mesh.shape["ep"], mesh.shape["tp"]
    body = build(ep, 4, tp // 2, 128, CW * tp, 14)
    return jax.shard_map(body, mesh=mesh, in_specs=SPECS_IN, out_specs=SPECS_OUT, check_vma=False)
```

```python
import functools

import jax
import jax.numpy as jnp
from jax import lax
from jax.experimental import pallas as pl
from jax.experimental.pallas import tpu as pltpu
from jax.sharding import PartitionSpec as P

BF = jnp.bfloat16
F32 = jnp.float32
CW = 128
SUB = 112
VMEM_MB = 24
HI = lax.Precision.HIGHEST
NN = ((1,), (0,))
NT = ((1,), (1,))
TN = ((0,), (0,))


def dot(a, b, dims=NN, precision=None):
    return lax.dot_general(a, b, (dims, ((), ())), precision=precision, preferred_element_type=F32)


def iota(shape, dim):
    return lax.broadcasted_iota(jnp.int32, shape, dim)


def one_hot(mask, dtype=BF):
    return jnp.where(mask, 1.0, 0.0).astype(dtype)


def kernel(
    cfg,
    rt_h, rw_h, tok_h, cot_h, gw_h, uw_h, dw_h,
    tg_r, rg_o, rr_o, gg_o, ug_o, dg_o, rowf_s, drow_o,
    rt_v, rw_v, tok_v, cot_v, w_own, w_par, dn_v,
    sel_v, cmp_v, a_s, a_r, xa, za, wcol, acc_gu, acc_b,
    hid_v, gp_own, gp_par, tm_v, part_v, rs_s, rs_r, ret_s, ret_r,
    g_s, g_r, gf_r, zr_r, xr_r, row_v, rowd_r, rowy_r,
    ld_sem, a_send, a_recv, y_send, y_recv, d_send, d_recv, w_send, w_recv, gp_send, gp_recv,
    g_send, g_recv, gf_send, gf_recv, rs_send, rs_recv, ret_send, ret_recv,
    z_send, z_recv, x_send, x_recv, rd_send, rd_recv, ry_send, ry_recv, rf_send, rf_recv,
    t_send, t_recv, td_send, td_recv,
):
    EP, NX, NY, T, D, CAP, PC = cfg
    cur = [None]

    def mark(n):
        if cur[0] is not None:
            cur[0].__exit__(None, None, None)
        cur[0] = None
        if n:
            cur[0] = jax.named_scope(n)
            cur[0].__enter__()

    NZ = EP // NX
    TP = 2 * NY
    H = NY // 2
    ROWS = EP * CAP
    SLOTS = EP * PC
    NS = ROWS // SUB
    shift = PC.bit_length() - 1
    inv = 65536 // CAP + 1
    ep = lax.axis_index("ep")
    tp = lax.axis_index("tp")
    y = lax.div(tp, 2)
    c = lax.rem(tp, 2)
    zc = lax.div(ep, NX)
    xc = lax.rem(ep, NX)
    partner = {"tp": y * 2 + (1 - c)}

    def ydev(off):
        return {"tp": lax.rem(y + off + NY, NY) * 2 + c}

    def remote(src, dst, ss, rs, dev):
        return pltpu.make_async_remote_copy(
            src_ref=src, dst_ref=dst, send_sem=ss, recv_sem=rs, device_id=dev,
            device_id_type=pl.DeviceIdType.MESH,
        )

    def each(lo, hi, body):
        def step(i, carry):
            body(i)
            return carry

        lax.fori_loop(lo, hi, step, 0)

    mark('load')
    barrier = pltpu.get_barrier_semaphore()

    xs_of = [lax.rem(xc + NX // 2 + (j + 1) // 2 * (1 - 2 * (j % 2)), NX) for j in range(NX)]

    def y_order(k):
        return H + lax.div(k + 1, 2) * (1 - 2 * lax.rem(k, 2))

    def each_peer(body):
        def plane(k):
            dz = NZ // 2 + lax.div(k + 1, 2) * (1 - 2 * lax.rem(k, 2))
            base = lax.rem(zc + dz, NZ) * NX
            for x in xs_of:
                body(base + x)

        each(0, NZ - 1, plane)
        for x in xs_of[:-1]:
            body(zc * NX + x)

    def settle(ref, sem):
        pltpu.make_async_copy(ref, ref, sem).wait()

    def greet_ep(peer):
        pl.semaphore_signal(barrier, inc=1, device_id={"ep": peer}, device_id_type=pl.DeviceIdType.MESH)

    def greet_tp(d):
        pl.semaphore_signal(barrier, inc=1, device_id={"tp": lax.rem(tp + d, TP)},
                            device_id_type=pl.DeviceIdType.MESH)

    each_peer(greet_ep)
    each(1, TP, greet_tp)
    ld_rt = pltpu.make_async_copy(rt_h, rt_v, ld_sem.at[5])
    ld_rw = pltpu.make_async_copy(rw_h, rw_v, ld_sem.at[6])
    ld_tok = pltpu.make_async_copy(tok_h, tok_v, ld_sem.at[0])
    ld_cot = pltpu.make_async_copy(cot_h, cot_v, ld_sem.at[1])
    ld_g = pltpu.make_async_copy(gw_h.at[0], w_own.at[0], ld_sem.at[2])
    ld_u = pltpu.make_async_copy(uw_h.at[0], w_own.at[1], ld_sem.at[3])
    ld_d = pltpu.make_async_copy(dw_h.at[0], dn_v, ld_sem.at[4])
    for cp in (ld_rt, ld_tok, ld_rw, ld_cot, ld_g, ld_u, ld_d):
        cp.start()

    mark('tables')
    ld_rt.wait()
    e_row = iota((EP, T), 0)
    hit_t = one_hot((e_row == rt_v[0:1, :]) | (e_row == rt_v[1:2, :]))
    hit = dot(hit_t, one_hot(iota((EP, EP), 0) == iota((EP, EP), 1)), TN).astype(BF)
    earlier = one_hot(iota((T, T), 1) < iota((T, T), 0))
    count = dot(earlier, hit).astype(BF)
    spread = one_hot((iota((EP, SLOTS), 1) >> shift) == iota((EP, SLOTS), 0))
    slot_lane = (iota((T, SLOTS), 1) & (PC - 1)).astype(F32)
    sel = jnp.where((dot(count, spread) == slot_lane) & (dot(hit, spread) > 0.5), 1.0, 0.0)
    sel_v[...] = sel.astype(BF)
    lane_of = one_hot((iota((SLOTS, CW), 0) & (PC - 1)) == iota((SLOTS, CW), 1))
    tail = one_hot(
        ((iota((SLOTS, EP), 0) >> shift) == iota((SLOTS, EP), 1))
        & ((iota((SLOTS, EP), 0) & (PC - 1)) == CAP)
    )
    row_id = iota((ROWS, SLOTS), 0)
    row_src = (row_id * inv) >> 16
    cmp_v[...] = one_hot(iota((ROWS, SLOTS), 1) == row_id + (PC - CAP) * row_src)

    ld_tok.wait()
    ld_rw.wait()
    affinity = jax.nn.sigmoid(dot(tok_v[...], rw_v[...], NT))
    hit32 = hit.astype(F32)
    chosen = affinity * hit32
    total = jnp.sum(chosen, axis=1, keepdims=True)
    weights = chosen / total
    wx = dot(weights.astype(BF), spread)
    slot_w = jnp.sum(sel * wx, axis=0, keepdims=True)
    w_rows = dot((spread.astype(F32) * slot_w).astype(BF), lane_of)
    sel_b = sel.astype(BF)

    def at(off):
        return lax.rem(y + off + NY, NY)

    def col_ds(chip):
        return pl.ds(pl.multiple_of((chip * 2 + c) * CW, CW), CW)

    cols = col_ds(y)
    extra = ((0, y), (1, y), (0, at(H)), (1, at(H)), (0, at(H - 1)), (1, at(1 - H)))
    ld_cot.wait()

    def fill(k):
        kind, chip = extra[k]
        val = dot(sel_b, (tok_v if kind == 0 else cot_v)[:, col_ds(chip)], TN)
        if k == 0:
            val = val + dot(tail, w_rows.astype(BF))
        a_s[k] = val.astype(BF).reshape(EP, PC, CW)
        a_r[k, ep] = a_s[k, ep]

    for k in range(6):
        fill(k)
    mark('barrier')
    pl.semaphore_wait(barrier, EP - 1 + TP - 1)

    mark('a2a_issue')

    def a2a(k, peer):
        return remote(a_s.at[k, peer], a_r.at[k, ep], a_send.at[k], a_recv.at[k], {"ep": peer})

    each_peer(lambda p: a2a(0, p).start())
    each_peer(lambda p: a2a(1, p).start())
    for k in range(2, 6):
        each_peer(lambda p, k=k: a2a(k, p).start())
    ld_g.wait()
    ld_u.wait()
    ld_d.wait()
    cp_w = remote(w_own, w_par, w_send, w_recv, partner)
    cp_w.start()

    bufs = (xa, za)

    def hop(way, step, part, src):
        blk = bufs[part].at[src, c]
        return remote(blk, blk, y_send, y_recv.at[way, step - 1, part],
                      ydev(1 if way == 0 else -1))

    def cross(part, src):
        blk = bufs[part].at[src, c]
        return remote(blk, blk, d_send, d_recv.at[part, src], partner)

    def cross_wait(part, src):
        blk = bufs[part].at[src, 1 - c]
        remote(blk, blk, d_send, d_recv.at[part, src], partner).wait_recv()

    def parts_of(way, step):
        return (0, 1) if step < H - 1 else ((0,) if way == 0 else (1,))

    def take(k):
        kind, chip = extra[k]
        settle(a_r.at[k, pl.ds(0, EP - 1)], a_recv.at[k])
        bufs[kind][chip, c] = dot(cmp_v[...], a_r[k].reshape(SLOTS, CW)).astype(BF)
        cross(kind, chip).start()

    for k in (0, 1):
        mark(f'a2a_wait{k}')
        take(k)
        for way in (0, 1):
            if k in parts_of(way, 1):
                hop(way, 1, k, y).start()
    rx_all = a_r[0].reshape(SLOTS, CW)

    mark('wcol')
    pick = one_hot(
        iota((ROWS, SLOTS), 1) == (row_src * PC + CAP)
    )
    w_sel = dot(pick, rx_all)
    r2 = iota((ROWS, CW), 0)
    r2_pos = r2 - ((r2 * inv) >> 16) * CAP
    w_masked = jnp.where(r2_pos == iota((ROWS, CW), 1), w_sel, 0.0)
    wcol[...] = jnp.broadcast_to(jnp.sum(w_masked, axis=1, keepdims=True), (ROWS, CW))

    acc_gu[...] = jnp.zeros_like(acc_gu)
    acc_b[...] = jnp.zeros_like(acc_b)

    def chunk_ds(src):
        return pl.ds(pl.multiple_of(src * 2 * CW, 2 * CW), 2 * CW)

    def forward_chunk(src):
        cross_wait(0, src)
        xs = jnp.concatenate([xa[src, 0], xa[src, 1]], axis=1)
        ds = chunk_ds(src)
        wgu = jnp.concatenate([w_own[0, ds, :], w_own[1, ds, :]], axis=1)
        acc_gu[...] += dot(xs, wgu)
        cross_wait(1, src)
        zs = jnp.concatenate([za[src, 0], za[src, 1]], axis=1)
        acc_b[...] += dot(zs, dn_v[:, ds], NT)

    mark('fwd0')
    each(0, 1, lambda i: forward_chunk(at(i)))
    for s in range(1, H):
        mark(f'gather{s}')
        for part in (0, 1):
            for way in (0, 1):
                if part not in parts_of(way, s):
                    continue
                src = at(-s if way == 0 else s)
                hop(way, s, part, src).wait_recv()
                if s < H - 1 and part in parts_of(way, s + 1):
                    hop(way, s + 1, part, src).start()
                cross(part, src).start()
        mark(f'fwd{s}')
        if s < H - 1:
            each(0, 2, lambda i, s=s: forward_chunk(at((2 * i - 1) * s)))
        if s == max(1, H - 2):
            mark('extra')
            take(2)
            take(3)
            each(0, 1, lambda i: forward_chunk(at(H + i)))
            take(4)
            take(5)
    mark('fwdL')
    each(0, 2, lambda i: forward_chunk(at((2 * i - 1) * (H - 1))))

    mark('pointwise')
    RB = 32 if ROWS % 64 == 0 and (ROWS // 2) % 32 == 0 else 16

    def pointwise(i):
        ds = pl.ds(pl.multiple_of(i * RB, RB), RB)
        pg = acc_gu[ds, :CW]
        pu = acc_gu[ds, CW:]
        bk = acc_b[ds, :]
        s = jax.nn.sigmoid(pg)
        hid = (pg * s * pu).astype(BF)
        hid_v[ds, :] = hid
        term = jnp.sum(hid.astype(F32) * bk, axis=1, keepdims=True)
        rr = iota((RB, CW), 0) + i * RB
        pos = rr - ((rr * inv) >> 16) * CAP
        tm_v[ds, :] = jnp.where(pos == iota((RB, CW), 1), term, 0.0)
        sc = wcol[ds, :] * bk
        gp_own[ds, :CW] = (sc * pu * s * (1.0 + pg * (1.0 - s))).astype(BF)
        gp_own[ds, CW:] = (sc * pg * s).astype(BF)

    HR = ROWS // 2

    def cp_gp(h):
        ds = pl.ds(h * HR, HR)
        return remote(gp_own.at[ds], gp_par.at[ds], gp_send.at[h], gp_recv.at[h], partner)

    for h in (0, 1):
        each(h * (HR // RB), (h + 1) * (HR // RB), pointwise)
        cp_gp(h).start()

    mark('gpwait')
    def weight_rows(w_v, off):
        ds = pl.ds(pl.multiple_of(at(off) * 2 * CW + c * CW, CW), CW)
        return jnp.concatenate([w_v[0, ds, :], w_v[1, ds, :]], axis=1)

    def partial_for(off):
        return dot(gp_own[...], weight_rows(w_own, off), NT) + dot(gp_par[...], weight_rows(w_par, off), NT)

    def rs(way, step, i):
        ds = pl.ds(i * SUB, SUB)
        return remote(rs_s.at[way * H + step - 1, ds], rs_r.at[way * H + step - 1, ds],
                      rs_send, rs_recv.at[way, step - 1, i],
                      ydev(1 if way == 0 else -1))

    def subs(way, step):
        if step > 1:
            return tuple(range(NS))
        return tuple(range(NS // 2, NS)) if way == 0 else tuple(range(NS // 2))

    own_first = dot(gp_own[...], weight_rows(w_own, H), NT)
    cp_w.wait_recv()
    for h in (0, 1):
        way = 1 - h
        ds = pl.ds(h * HR, HR)
        cp_gp(h).wait_recv()
        val = own_first[h * HR:(h + 1) * HR] + dot(gp_par[ds, :], weight_rows(w_par, H), NT)
        rs_s[way * H, ds] = val.astype(BF)
        for i in subs(way, 1):
            rs(way, 1, i).start()

    def own_parts(step):
        part_v[0] = partial_for(H - step + 1)
        part_v[1] = partial_for(-(H - step + 1))

    def rs_step(step):
        have = [(i, w) for i in range(NS) for w in (0, 1)]
        have.sort(key=lambda t: (t[0] in subs(t[1], step - 1)))
        for i, w in have:
            ds = pl.ds(i * SUB, SUB)
            val = part_v[w, ds, :]
            if i in subs(w, step - 1):
                rs(w, step - 1, i).wait_recv()
                val = val + rs_r[w * H + step - 2, ds, :].astype(F32)
            rs_s[w * H + step - 1, ds, :] = val.astype(BF)
            rs(w, step, i).start()

    mark('gterm')
    block_of = one_hot(((iota((EP, ROWS), 1) * inv) >> 16) == iota((EP, ROWS), 0), F32)
    g_s[...] = dot(block_of, tm_v[...], NN, HI).reshape(EP, 1, CW)
    g_r[ep] = g_s[ep]

    def g_copy(peer, slot):
        return remote(g_s.at[peer], g_r.at[slot], g_send, g_recv, {"ep": peer})

    each_peer(lambda p: g_copy(p, ep).start())

    ones = jnp.ones((8, 2 * CW), BF)

    def grads(src):
        ds = chunk_ds(src)
        xs = jnp.concatenate([xa[src, 0], xa[src, 1]], axis=1)
        gu = dot(xs, gp_own[...], TN)
        gg_o[ds, :] = gu[:, :CW].astype(BF)
        ug_o[ds, :] = gu[:, CW:].astype(BF)
        sq = (gu * gu).astype(BF)
        for k in (0, 1):
            tot = dot(ones[:, :CW], sq[:, k * CW:(k + 1) * CW], NT)
            row_v[k, pl.ds(src * 2, 1)] = tot[0:1, :CW].reshape(1, 1, CW)
            row_v[k, pl.ds(src * 2 + 1, 1)] = tot[0:1, CW:].reshape(1, 1, CW)

    def down_grads(src):
        ds = chunk_ds(src)
        scale = wcol[...]
        w0 = (scale * za[src, 0].astype(F32)).astype(BF)
        w1 = (scale * za[src, 1].astype(F32)).astype(BF)
        dgr = dot(hid_v[...], jnp.concatenate([w0, w1], axis=1), TN)
        dg_o[:, ds] = dgr.astype(BF)
        drow_o[...] += dot(ones, (dgr * dgr).astype(BF), NT)[0:1]

    def flatten_terms():
        mark('gflat')
        settle(g_r.at[pl.ds(0, EP - 1)], g_recv)
        lane_t = one_hot((iota((CW, SLOTS), 1) & (PC - 1)) == iota((CW, SLOTS), 0), F32)
        spread32 = one_hot((iota((EP, SLOTS), 1) >> shift) == iota((EP, SLOTS), 0), F32)
        g_flat = jnp.sum(dot(g_r[...].reshape(EP, CW), lane_t, NN, HI) * spread32, axis=0, keepdims=True)
        gf_r[tp] = g_flat

        def gf(peer, slot):
            return remote(gf_r.at[tp], gf_r.at[slot], gf_send, gf_recv, {"tp": peer})

        def tpeer(d):
            return lax.rem(tp + d, TP)

        each(1, TP, lambda d: gf(tpeer(d), tp).start())

    mark('own2')
    own_parts(2)
    mark('rs2')
    rs_step(2)
    done = 0
    for step in range(3, H + 1):
        mark(f'own{step}')
        own_parts(step)
        each(done, done + 1, grads)
        done += 1
        mark(f'rs{step}')
        rs_step(step)
        if step == 3:
            flatten_terms()
    if H < 3:
        flatten_terms()

    mark('rsfinal')
    own = partial_for(0)
    BPS = SUB // CAP

    def ret(peer, slot):
        return remote(ret_s.at[peer], ret_r.at[slot], ret_send, ret_recv, {"ep": peer})

    for i in range(NS):
        ds = pl.ds(i * SUB, SUB)
        val = own[i * SUB:(i + 1) * SUB]
        for w in (0, 1):
            rs(w, H, i).wait_recv()
            val = val + rs_r[w * H + H - 1, ds, :].astype(F32)
        spread_rows = cmp_v[ds, i * BPS * PC:(i + 1) * BPS * PC]
        ret_s[i * BPS:(i + 1) * BPS] = dot(spread_rows, val.astype(BF), TN).astype(BF).reshape(BPS, PC, CW)

        def send_back(b):
            @pl.when(b != ep)
            def _():
                ret(b, ep).start()

        each(i * BPS, (i + 1) * BPS, send_back)
    ret_r[ep] = ret_s[ep]

    mark('router')
    settle(gf_r.at[pl.ds(0, TP - 1)], gf_recv)
    g_tot = gf_r[0]
    for j in range(1, TP):
        g_tot = g_tot + gf_r[j]
    g_tot = g_tot.astype(BF).astype(F32)
    d_w = dot((sel_v[...].astype(F32) * g_tot).astype(BF), one_hot(
        (iota((SLOTS, EP), 0) >> shift) == iota((SLOTS, EP), 1)))
    d_chosen = (d_w - jnp.sum(d_w * weights, axis=1, keepdims=True)) / total
    d_logits = (d_chosen * chosen * (1.0 - affinity) * hit32).astype(BF)
    tok_c = tok_v[:, cols]
    zr_r[zc] = dot(d_logits, tok_c, TN)

    def zdev(off):
        return {"ep": lax.rem(zc + off, NZ) * NX + xc}

    def zsend(d):
        return remote(zr_r.at[zc], zr_r.at[zc], z_send, z_recv, zdev(d))

    each(1, NZ, lambda d: zsend(d).start())

    mark('gradsL')
    each(done, NY, grads)
    mark('rownorm')

    def rowd(k):
        return remote(row_v.at[k], rowd_r, rd_send, rd_recv, partner)

    rowd(1 - c).start()

    rd_wait = rowd(1 - c)

    router_back = dot(d_logits, rw_v[:, cols])

    mark('rdwait')
    rd_wait.wait_recv()
    rowy_r[y] = row_v[c] + rowd_r[...]

    def ry(d):
        return remote(rowy_r.at[y], rowy_r.at[y], ry_send, ry_recv, ydev(d))

    each(1, NY, lambda d: ry(d).start())

    mark('retwait')
    settle(ret_r.at[pl.ds(0, EP - 1)], ret_recv)
    mark('combine')
    back = dot(sel_v[...], ret_r[...].reshape(SLOTS, CW))
    tg_r[y, c] = (back + router_back).astype(BF)

    def tg(d):
        blk = tg_r.at[y, c]
        return remote(blk, blk, t_send, t_recv.at[y], ydev(d))

    def tg_wait(d):
        blk = tg_r.at[at(d), c]
        remote(blk, blk, t_send, t_recv.at[at(d)], ydev(d)).wait_recv()

    def tgd(src):
        blk = tg_r.at[src, c]
        return remote(blk, blk, td_send, td_recv, partner)

    each(0, NY - 1, lambda k: tg(y_order(k)).start())
    tgd(y).start()

    mark('zwait')
    settle(zr_r.at[pl.ds(0, NZ - 1)], z_recv)
    z_tot = zr_r[0]
    for j in range(1, NZ):
        z_tot = z_tot + zr_r[j]
    xr_r[xc] = z_tot

    def xdev(off):
        return {"ep": zc * NX + lax.rem(xc + off, NX)}

    def xsend(d):
        return remote(xr_r.at[xc], xr_r.at[xc], x_send, x_recv, xdev(d))

    each(1, NX, lambda d: xsend(d).start())
    mark('rywait')
    settle(rowy_r.at[pl.ds(0, NY - 1)], ry_recv)
    r_tot = rowy_r[0]
    for j in range(1, NY):
        r_tot = r_tot + rowy_r[j]
    rowf_s[c] = r_tot
    rf = remote(rowf_s.at[c], rowf_s.at[c], rf_send, rf_recv, partner)
    rf.start()
    mark('down')
    drow_o[...] = jnp.zeros_like(drow_o)
    each(0, NY, down_grads)
    mark('xwait')
    if NX > 1:
        settle(xr_r.at[pl.ds(0, NX - 1)], x_recv)
    x_tot = xr_r[0]
    for j in range(1, NX):
        x_tot = x_tot + xr_r[j]
    rg_o[...] = x_tot
    rr_o[...] = jnp.sum(x_tot * x_tot, axis=0, keepdims=True)

    mark('drain')
    for k in range(6):
        settle(a_s.at[k, pl.ds(0, EP - 1)], a_send.at[k])
    settle(g_s.at[pl.ds(0, EP - 1)], g_send)
    settle(ret_s.at[pl.ds(0, EP - 1)], ret_send)
    settle(gf_r.at[pl.ds(0, TP - 1)], gf_send)
    settle(zr_r.at[pl.ds(0, NZ - 1)], z_send)
    if NX > 1:
        settle(xr_r.at[pl.ds(0, NX - 1)], x_send)
    settle(rowy_r.at[pl.ds(0, NY - 1)], ry_send)
    settle(xa, d_send)
    settle(xa.at[pl.ds(0, 2 * H - 3)], y_send)
    settle(rs_s.at[pl.ds(0, 2 * H - 1)], rs_send)
    cp_w.wait_send()
    for h in (0, 1):
        cp_gp(h).wait_send()
    rd_wait.wait_send()
    remote(rowf_s.at[1 - c], rowf_s.at[1 - c], rf_send, rf_recv, partner).wait_recv()
    rf.wait_send()

    mark('agwait')

    def arrive(k):
        d = y_order(NY - 2 - k)
        tg_wait(d)
        tgd(at(d)).start()

    each(0, NY - 1, arrive)
    mark('agd')
    settle(tg_r.at[pl.ds(0, NY - 1), c], t_send)
    settle(tg_r.at[:, 1 - c], td_recv)
    settle(tg_r.at[:, c], td_send)
    mark(None)


def place(ny, tg, rg, rr, gg, ug, dg, rows, drow, tg_o, rg_o, rr_o, gg_o, ug_o, dg_o, gr_o, ur_o, drow_o, sem):
    pairs = [(gg, gg_o.at[0]), (ug, ug_o.at[0]), (dg, dg_o.at[0]), (rg, rg_o), (rr, rr_o),
             (rows.at[0], gr_o), (rows.at[1], ur_o), (drow, drow_o)]
    for j in range(ny):
        for k in (0, 1):
            pairs.append((tg.at[j, k], tg_o.at[:, pl.ds((2 * j + k) * CW, CW)]))
    copies = [pltpu.make_async_copy(a, b, sem.at[i]) for i, (a, b) in enumerate(pairs)]
    for cp in copies:
        cp.start()
    for cp in copies:
        cp.wait()


def build(ep, nx, ny, tok, width, cap):
    pc = 1
    while pc <= cap:
        pc *= 2
    rows, slots, tp, half = ep * cap, ep * pc, 2 * ny, ny // 2
    ns = rows // SUB
    hb = width // CW
    nz = ep // nx
    cfg = (ep, nx, ny, tok, width, cap, pc)
    v = pltpu.VMEM
    dma = pltpu.SemaphoreType.DMA
    scratch = [
        v((2, tok), jnp.int32), v((ep, width), BF),
        v((tok, width), BF), v((tok, width), BF), v((2, width, CW), BF), v((2, width, CW), BF), v((CW, width), BF),
        v((tok, slots), BF), v((rows, slots), BF),
        v((6, ep, pc, CW), BF), v((6, ep, pc, CW), BF),
        v((ny, 2, rows, CW), BF), v((ny, 2, rows, CW), BF),
        v((rows, CW), F32), v((rows, 2 * CW), F32), v((rows, CW), F32),
        v((rows, CW), BF), v((rows, 2 * CW), BF), v((rows, 2 * CW), BF), v((rows, CW), F32),
        v((2, rows, CW), F32), v((2 * half, rows, CW), BF), v((2 * half, rows, CW), BF),
        v((ep, pc, CW), BF), v((ep, pc, CW), BF),
        v((ep, 1, CW), F32), v((ep, 1, CW), F32), v((tp, 1, slots), F32),
        v((nz, ep, CW), F32), v((nx, ep, CW), F32),
        v((2, hb, 1, CW), F32), v((hb, 1, CW), F32), v((ny, hb, 1, CW), F32),
        dma((7,)), dma((6,)), dma((6,)), dma, dma((2, half, 2)), dma, dma((2, ny)), dma, dma, dma((2,)), dma((2,)),
        dma, dma, dma, dma, dma, dma((2, half, ns)), dma, dma, dma, dma, dma, dma, dma, dma, dma, dma, dma, dma,
        dma, dma((ny,)), dma, dma,
    ]
    sds = jax.ShapeDtypeStruct
    out_shape = (
        sds((ny, 2, tok, CW), BF), sds((ep, CW), F32), sds((1, CW), F32),
        sds((width, CW), BF), sds((width, CW), BF), sds((CW, width), BF),
        sds((2, hb, 1, CW), F32), sds((1, CW), F32),
    )
    vm = pl.BlockSpec(memory_space=pltpu.VMEM)
    hbm = pl.BlockSpec(memory_space=pltpu.HBM)
    anywhere = pl.BlockSpec(memory_space=pl.ANY)
    call = pl.pallas_call(
        functools.partial(kernel, cfg),
        out_shape=out_shape,
        in_specs=[hbm] * 7,
        out_specs=tuple([vm] * 8),
        scratch_shapes=scratch,
        compiler_params=pltpu.CompilerParams(
            collective_id=0, has_side_effects=True, vmem_limit_bytes=VMEM_MB * 1024 * 1024
        ),
        name="experts_backward",
    )
    finish = pl.pallas_call(
        functools.partial(place, ny),
        out_shape=(
            sds((tok, width), BF), sds((ep, CW), F32), sds((1, CW), F32),
            sds((1, width, CW), BF), sds((1, width, CW), BF), sds((1, CW, width), BF),
            sds((hb, 1, CW), F32), sds((hb, 1, CW), F32), sds((1, CW), F32),
        ),
        in_specs=[anywhere] * 8,
        out_specs=tuple([hbm] * 9),
        scratch_shapes=[dma((2 * ny + 8,))],
        compiler_params=pltpu.CompilerParams(vmem_limit_bytes=1024 * 1024),
        name="place_outputs",
    )

    def per_device(tokens, routing, router_weight, gate_weight, up_weight, down_weight, cotangent):
        args = (routing.T, router_weight.T, tokens, cotangent, gate_weight, up_weight, down_weight)
        parts = call(*[pltpu.with_memory_space_constraint(a, pltpu.HBM) for a in args])
        tg, rg, rr, gg, ug, dg, gr, ur, drow = finish(*parts)
        return (
            tg, rg.T, rr.reshape(CW), gg, ug, dg, gr.reshape(1, width), ur.reshape(1, width), drow,
        )

    return per_device


SPECS_IN = (
    P("ep", None), P("ep", None), P(), P("ep", None, "tp"), P("ep", None, "tp"), P("ep", "tp", None), P("ep", None),
)
SPECS_OUT = (
    P("ep", None), P("tp", None), P("tp"), P("ep", None, "tp"), P("ep", None, "tp"), P("ep", "tp", None),
    P("ep", None), P("ep", None), P("ep", "tp"),
)


def solution(mesh):
    ep, tp = mesh.shape["ep"], mesh.shape["tp"]
    body = build(ep, 4, tp // 2, 128, CW * tp, 14)
    return jax.shard_map(body, mesh=mesh, in_specs=SPECS_IN, out_specs=SPECS_OUT, check_vma=False)
```

```python
import functools

import jax
import jax.numpy as jnp
from jax import lax
from jax.experimental import pallas as pl
from jax.experimental.pallas import tpu as pltpu
from jax.sharding import PartitionSpec as P

BF = jnp.bfloat16
F32 = jnp.float32
CW = 128
SUB = 112
VMEM_MB = 24
HI = lax.Precision.HIGHEST
NN = ((1,), (0,))
NT = ((1,), (1,))
TN = ((0,), (0,))


def dot(a, b, dims=NN, precision=None):
    return lax.dot_general(a, b, (dims, ((), ())), precision=precision, preferred_element_type=F32)


def iota(shape, dim):
    return lax.broadcasted_iota(jnp.int32, shape, dim)


def one_hot(mask, dtype=BF):
    return jnp.where(mask, 1.0, 0.0).astype(dtype)


def kernel(
    cfg,
    rt_h, rw_h, tok_h, cot_h, gw_h, uw_h, dw_h,
    tg_r, rg_o, rr_o, gg_o, ug_o, dg_o, rowf_s, drow_o,
    rt_v, rw_v, tok_v, cot_v, w_own, w_par, dn_v,
    sel_v, cmp_v, a_s, a_r, xa, za, wcol, acc_gu, acc_b,
    hid_v, gp_own, gp_par, tm_v, part_v, own_v, rs_s, rs_r, ret_s, ret_r,
    g_s, g_r, gf_r, zr_s, zr_r, xr_r, row_v, rowd_r, rowy_r, e_s, e_r, fw_s, fw_r,
    ld_sem, a_send, a_recv, y_send, y_recv, d_send, d_recv, w_send, w_recv, gp_send, gp_recv,
    g_send, g_recv, gf_send, gf_recv, rs_send, rs_recv, ret_send, ret_recv,
    z_send, z_recv, x_send, x_recv, rd_send, rd_recv, ry_send, ry_recv, rf_send, rf_recv,
    t_send, t_recv, td_send, td_recv, e_send, e_recv, fw_send, fw_recv,
):
    EP, NX, NY, T, D, CAP, PC = cfg
    cur = [None]

    def mark(n):
        if cur[0] is not None:
            cur[0].__exit__(None, None, None)
        cur[0] = None
        if n:
            cur[0] = jax.named_scope(n)
            cur[0].__enter__()

    NZ = EP // NX
    TP = 2 * NY
    H = NY // 2
    ROWS = EP * CAP
    SLOTS = EP * PC
    NS = ROWS // SUB
    shift = PC.bit_length() - 1
    inv = 65536 // CAP + 1
    ep = lax.axis_index("ep")
    tp = lax.axis_index("tp")
    y = lax.div(tp, 2)
    c = lax.rem(tp, 2)
    zc = lax.div(ep, NX)
    xc = lax.rem(ep, NX)
    other = 1 - c
    partner = {"tp": y * 2 + other}

    def ydev(off):
        return {"tp": lax.rem(y + off + NY, NY) * 2 + c}

    def ydev_x(off):
        return {"tp": lax.rem(y + off + NY, NY) * 2 + other}

    def home(peer):
        return {"ep": peer, "tp": y * 2 + other}

    def core_at(dist):
        return other if dist % 2 else c

    def remote(src, dst, ss, rs, dev):
        return pltpu.make_async_remote_copy(
            src_ref=src, dst_ref=dst, send_sem=ss, recv_sem=rs, device_id=dev,
            device_id_type=pl.DeviceIdType.MESH,
        )

    def each(lo, hi, body):
        def step(i, carry):
            body(i)
            return carry

        lax.fori_loop(lo, hi, step, 0)

    mark('load')
    barrier = pltpu.get_barrier_semaphore()

    xs_of = [lax.rem(xc + NX // 2 + (j + 1) // 2 * (1 - 2 * (j % 2)), NX) for j in range(NX)]

    def y_order(k):
        return H + lax.div(k + 1, 2) * (1 - 2 * lax.rem(k, 2))

    def each_peer(body):
        def plane(k):
            dz = NZ // 2 + lax.div(k + 1, 2) * (1 - 2 * lax.rem(k, 2))
            base = lax.rem(zc + dz, NZ) * NX
            for x in xs_of:
                body(base + x)

        each(0, NZ - 1, plane)
        for x in xs_of[:-1]:
            body(zc * NX + x)

    def settle(ref, sem):
        pltpu.make_async_copy(ref, ref, sem).wait()

    def each_home(body):
        each_peer(body)
        body(ep)

    def greet_ep(peer):
        pl.semaphore_signal(barrier, inc=1, device_id=home(peer), device_id_type=pl.DeviceIdType.MESH)

    def greet_x(peer):
        pl.semaphore_signal(barrier, inc=1, device_id={"ep": peer}, device_id_type=pl.DeviceIdType.MESH)

    def greet_tp(d):
        pl.semaphore_signal(barrier, inc=1, device_id={"tp": lax.rem(tp + d, TP)},
                            device_id_type=pl.DeviceIdType.MESH)

    each_peer(greet_ep)
    for x in xs_of[:-1]:
        greet_x(zc * NX + x)
    each(1, TP, greet_tp)
    ld_rt = pltpu.make_async_copy(rt_h, rt_v, ld_sem.at[5])
    ld_rw = pltpu.make_async_copy(rw_h, rw_v, ld_sem.at[6])
    ld_tok = pltpu.make_async_copy(tok_h, tok_v, ld_sem.at[0])
    ld_cot = pltpu.make_async_copy(cot_h, cot_v, ld_sem.at[1])
    ld_g = pltpu.make_async_copy(gw_h.at[0], w_own.at[0], ld_sem.at[2])
    ld_u = pltpu.make_async_copy(uw_h.at[0], w_own.at[1], ld_sem.at[3])
    ld_d = pltpu.make_async_copy(dw_h.at[0], dn_v, ld_sem.at[4])
    for cp in (ld_rt, ld_tok, ld_rw, ld_cot, ld_g, ld_u, ld_d):
        cp.start()

    mark('tables')
    ld_rt.wait()
    e_row = iota((EP, T), 0)
    hit_t = one_hot((e_row == rt_v[0:1, :]) | (e_row == rt_v[1:2, :]))
    hit = dot(hit_t, one_hot(iota((EP, EP), 0) == iota((EP, EP), 1)), TN).astype(BF)
    earlier = one_hot(iota((T, T), 1) < iota((T, T), 0))
    count = dot(earlier, hit).astype(BF)
    spread = one_hot((iota((EP, SLOTS), 1) >> shift) == iota((EP, SLOTS), 0))
    slot_lane = (iota((T, SLOTS), 1) & (PC - 1)).astype(F32)
    sel = jnp.where((dot(count, spread) == slot_lane) & (dot(hit, spread) > 0.5), 1.0, 0.0)
    sel_v[...] = sel.astype(BF)
    lane_of = one_hot((iota((SLOTS, CW), 0) & (PC - 1)) == iota((SLOTS, CW), 1))
    tail = one_hot(
        ((iota((SLOTS, EP), 0) >> shift) == iota((SLOTS, EP), 1))
        & ((iota((SLOTS, EP), 0) & (PC - 1)) == CAP)
    )
    row_id = iota((ROWS, SLOTS), 0)
    row_src = (row_id * inv) >> 16
    cmp_v[...] = one_hot(iota((ROWS, SLOTS), 1) == row_id + (PC - CAP) * row_src)

    ld_tok.wait()
    ld_rw.wait()
    affinity = jax.nn.sigmoid(dot(tok_v[...], rw_v[...], NT))
    hit32 = hit.astype(F32)
    chosen = affinity * hit32
    total = jnp.sum(chosen, axis=1, keepdims=True)
    weights = chosen / total
    wx = dot(weights.astype(BF), spread)
    slot_w = jnp.sum(sel * wx, axis=0, keepdims=True)
    w_rows = dot((spread.astype(F32) * slot_w).astype(BF), lane_of)
    sel_b = sel.astype(BF)

    def at(off):
        return lax.rem(y + off + NY, NY)

    def col_ds(chip):
        return pl.ds(pl.multiple_of((chip * 2 + other) * CW, CW), CW)

    cols_x = col_ds(y)
    extra = ((0, y), (1, y), (0, at(H)), (1, at(H)), (1, at(H - 1)), (1, at(1 - H)))
    ld_cot.wait()

    def fill(k):
        kind, chip = extra[k]
        val = dot(sel_b, (tok_v if kind == 0 else cot_v)[:, col_ds(chip)], TN)
        if k == 0:
            val = val + dot(tail, w_rows.astype(BF))
        a_s[k] = val.astype(BF).reshape(EP, PC, CW)

    for k in range(6):
        fill(k)
    mark('barrier')
    pl.semaphore_wait(barrier, EP - 1 + NX - 1 + TP - 1)

    mark('a2a_issue')

    def a2a(k, peer):
        used = pl.ds(0, CAP if k else PC)
        return remote(a_s.at[k, peer, used], a_r.at[k, ep, used], a_send.at[k], a_recv.at[k], home(peer))

    def filled(tiles):
        return jnp.where(iota((EP, PC, CW), 1) < CAP, tiles, jnp.zeros_like(tiles)).reshape(SLOTS, CW)

    each_home(lambda p: a2a(0, p).start())
    each_home(lambda p: a2a(1, p).start())
    for k in range(2, 6):
        each_home(lambda p, k=k: a2a(k, p).start())
    ld_g.wait()
    ld_u.wait()
    ld_d.wait()
    cp_w = remote(w_own, w_par, w_send, w_recv, partner)
    cp_w.start()

    bufs = (xa, za)

    def hop(way, step, part, src, sending=True):
        blk = bufs[part].at[src, core_at(step - 1 if sending else step)]
        return remote(blk, blk, y_send, y_recv.at[way, step - 1, part], ydev_x(1 if way == 0 else -1))

    def cross(part, src, core):
        blk = bufs[part].at[src, core]
        return remote(blk, blk, d_send, d_recv.at[part, src], partner)

    def cross_wait(part, src):
        cross(part, src, c).wait_recv()

    def parts_of(way, step):
        return (0, 1) if step < H - 1 else (0,)

    def take(k):
        kind, chip = extra[k]
        settle(a_r.at[k, :, pl.ds(0, CAP if k else PC)], a_recv.at[k])
        tiles = filled(a_r[k]) if k else a_r[k].reshape(SLOTS, CW)
        bufs[kind][chip, c] = dot(cmp_v[...], tiles).astype(BF)
        cross(kind, chip, c).start()

    for k in (0, 1):
        mark(f'a2a_wait{k}')
        take(k)
        for way in (0, 1):
            if k in parts_of(way, 1):
                hop(way, 1, k, y).start()
    rx_all = a_r[0].reshape(SLOTS, CW)

    mark('wcol')
    pick = one_hot(
        iota((ROWS, SLOTS), 1) == (row_src * PC + CAP)
    )
    w_sel = dot(pick, rx_all)
    r2 = iota((ROWS, CW), 0)
    r2_pos = r2 - ((r2 * inv) >> 16) * CAP
    w_masked = jnp.where(r2_pos == iota((ROWS, CW), 1), w_sel, 0.0)
    wcol[...] = jnp.broadcast_to(jnp.sum(w_masked, axis=1, keepdims=True), (ROWS, CW))

    acc_gu[...] = jnp.zeros_like(acc_gu)
    acc_b[...] = jnp.zeros_like(acc_b)

    def chunk_ds(src):
        return pl.ds(pl.multiple_of(src * 2 * CW, 2 * CW), 2 * CW)

    def forward_x(src):
        cross_wait(0, src)
        xs = jnp.concatenate([xa[src, 0], xa[src, 1]], axis=1)
        ds = chunk_ds(src)
        wgu = jnp.concatenate([w_own[0, ds, :], w_own[1, ds, :]], axis=1)
        acc_gu[...] += dot(xs, wgu)

    def forward_z(src):
        cross_wait(1, src)
        zs = jnp.concatenate([za[src, 0], za[src, 1]], axis=1)
        acc_b[...] += dot(zs, dn_v[:, chunk_ds(src)], NT)

    def forward_chunk(src):
        forward_x(src)
        forward_z(src)

    def receive(s, part):
        mark(f'gather{s}{part}')
        for way in (0, 1):
            if part in parts_of(way, s):
                src = at(-s if way == 0 else s)
                hop(way, s, part, src, False).wait_recv()
                if s < H - 1 and part in parts_of(way, s + 1):
                    hop(way, s + 1, part, src).start()
                cross(part, src, core_at(s)).start()
        mark(f'fwd{s}{part}')

    def both(s, body):
        each(0, 2, lambda i: body(at((2 * i - 1) * s)))

    def extra_part(k):
        mark(f'extra{k}')
        take(k)

    mark('fwd0')
    each(0, 1, lambda i: forward_chunk(at(i)))
    if H == 4:
        receive(1, 0)
        receive(1, 1)
        both(1, forward_x)
        extra_part(2)
        receive(2, 0)
        both(1, forward_z)
        extra_part(3)
        receive(2, 1)
        both(2, forward_x)
        each(0, 1, lambda i: forward_chunk(at(H + i)))
        extra_part(4)
        both(2, forward_z)
        extra_part(5)
        receive(3, 0)
        both(3, forward_z)
        both(3, forward_x)
    else:
        for k in range(2, 6):
            extra_part(k)
        each(0, 1, lambda i: forward_chunk(at(H + i)))
        for s in range(1, H):
            for part in (0, 1) if s < H - 1 else (0,):
                receive(s, part)
            both(s, forward_x)
            both(s, forward_z)

    mark('pointwise')
    RB = 32 if ROWS % 64 == 0 and (ROWS // 2) % 32 == 0 else 16

    def pointwise(i):
        ds = pl.ds(pl.multiple_of(i * RB, RB), RB)
        pg = acc_gu[ds, :CW]
        pu = acc_gu[ds, CW:]
        bk = acc_b[ds, :]
        s = jax.nn.sigmoid(pg)
        hid = (pg * s * pu).astype(BF)
        hid_v[ds, :] = hid
        term = jnp.sum(hid.astype(F32) * bk, axis=1, keepdims=True)
        rr = iota((RB, CW), 0) + i * RB
        pos = rr - ((rr * inv) >> 16) * CAP
        tm_v[ds, :] = jnp.where(pos == iota((RB, CW), 1), term, 0.0)
        sc = wcol[ds, :] * bk
        gp_own[ds, :CW] = (sc * pu * s * (1.0 + pg * (1.0 - s))).astype(BF)
        gp_own[ds, CW:] = (sc * pg * s).astype(BF)

    HR = ROWS // 2

    def cp_gp(h):
        ds = pl.ds(h * HR, HR)
        return remote(gp_own.at[ds], gp_par.at[ds], gp_send.at[h], gp_recv.at[h], partner)

    for h in (0, 1):
        lax.fori_loop(h * (HR // RB), (h + 1) * (HR // RB), lambda i, carry: (pointwise(i), carry)[1], 0, unroll=True)
        cp_gp(h).start()

    mark('gpwait')
    def weight_rows(w_v, off, core):
        ds = pl.ds(pl.multiple_of(at(off) * 2 * CW + core * CW, CW), CW)
        return jnp.concatenate([w_v[0, ds, :], w_v[1, ds, :]], axis=1)

    K = H - 1

    def pair_parts(off_a, off_b, core_a, core_b, own_only=False, rows=slice(None), prior=None):
        def side(w_v):
            return jnp.concatenate([weight_rows(w_v, off_a, core_a), weight_rows(w_v, off_b, core_b)], axis=0)

        first = dot(gp_own[rows, :], side(w_own), NT) if prior is None else prior
        return first if own_only else first + dot(gp_par[rows, :], side(w_par), NT)

    PPS = NZ // NS

    def sub_at(p):
        off = NS // 2 + (p + 1) // 2 * (1 - 2 * (p % 2))
        return lax.rem(lax.div(zc, PPS) + off, NS)

    sub_ids = [sub_at(p) for p in range(NS)]
    sub_ds = [pl.ds(pl.multiple_of(i * SUB, 16), SUB) for i in sub_ids]

    def rs(way, step, p):
        ds = sub_ds[p]
        return remote(rs_s.at[way * K + step - 1, ds], rs_r.at[way * K + step - 1, ds],
                      rs_send, rs_recv.at[way, step - 1, p],
                      ydev_x(1 if way == 0 else -1))

    own_first = pair_parts(K, -K, core_at(K), core_at(K), own_only=True)
    cp_w.wait_recv()
    for h in (0, 1):
        cp_gp(h).wait_recv()
    first_pair = pair_parts(K, -K, core_at(K), core_at(K), prior=own_first).astype(BF)
    for way in (0, 1):
        rs_s[way * K] = first_pair[:, way * CW:(way + 1) * CW]
    for p in range(NS):
        for way in (0, 1):
            rs(way, 1, p).start()

    def own_parts(step):
        part_v[...] = pair_parts(K - step + 1, step - K - 1, core_at(K - step + 1), core_at(K - step + 1))

    def rs_step(step, between):
        for i in range(NS):
            for w in (0, 1):
                ds = sub_ds[i]
                rs(w, step - 1, i).wait_recv()
                val = part_v[ds, w * CW:(w + 1) * CW] + rs_r[w * K + step - 2, ds, :].astype(F32)
                rs_s[w * K + step - 1, ds, :] = val.astype(BF)
                rs(w, step, i).start()
        between()

    mark('gterm')
    block_of = one_hot(((iota((EP, ROWS), 1) * inv) >> 16) == iota((EP, ROWS), 0), F32)
    g_s[...] = dot(block_of, tm_v[...], NN, HI).reshape(EP, 1, CW)

    def g_copy(peer, slot):
        return remote(g_s.at[peer], g_r.at[slot], g_send, g_recv, home(peer))

    each_home(lambda p: g_copy(p, ep).start())

    ones = jnp.ones((8, 2 * CW), BF)

    def grads(src):
        ds = chunk_ds(src)
        xs = jnp.concatenate([xa[src, 0], xa[src, 1]], axis=1)
        gu = dot(xs, gp_own[...], TN)
        gg_o[ds, :] = gu[:, :CW].astype(BF)
        ug_o[ds, :] = gu[:, CW:].astype(BF)
        sq = (gu * gu).astype(BF)
        for k in (0, 1):
            tot = dot(ones[:, :CW], sq[:, k * CW:(k + 1) * CW], NT)
            row_v[k, pl.ds(src * 2, 1)] = tot[0:1, :CW].reshape(1, 1, CW)
            row_v[k, pl.ds(src * 2 + 1, 1)] = tot[0:1, CW:].reshape(1, 1, CW)

    def down_grads(src):
        ds = chunk_ds(src)
        scale = wcol[...]
        w0 = (scale * za[src, 0].astype(F32)).astype(BF)
        w1 = (scale * za[src, 1].astype(F32)).astype(BF)
        dgr = dot(hid_v[...], jnp.concatenate([w0, w1], axis=1), TN)
        dg_o[:, ds] = dgr.astype(BF)
        drow_o[...] += dot(ones, (dgr * dgr).astype(BF), NT)[0:1]

    def flatten_terms():
        mark('gflat')
        settle(g_r, g_recv)
        lane_t = one_hot((iota((CW, SLOTS), 1) & (PC - 1)) == iota((CW, SLOTS), 0), F32)
        spread32 = one_hot((iota((EP, SLOTS), 1) >> shift) == iota((EP, SLOTS), 0), F32)
        g_flat = jnp.sum(dot(g_r[...].reshape(EP, CW), lane_t, NN, HI) * spread32, axis=0, keepdims=True)
        gf_r[tp] = g_flat

        def gf(peer, slot):
            return remote(gf_r.at[tp], gf_r.at[slot], gf_send, gf_recv, {"tp": peer})

        def tpeer(d):
            return lax.rem(tp + d, TP)

        each(1, TP, lambda d: gf(tpeer(d), tp).start())

    mark('own2')
    if K > 1:
        own_parts(2)
    mark('far')
    far_near = pair_parts(H, 0, other, c)
    own_v[...] = far_near[:, CW:]
    e_s[...] = dot(cmp_v[...], far_near[:, :CW].astype(BF), TN).astype(BF).reshape(EP, PC, CW)

    def far(peer):
        used = pl.ds(0, CAP)
        return remote(e_s.at[peer, used], e_r.at[ep, used], e_send, e_recv, home(peer))

    each_home(lambda p: far(p).start())
    done = 0
    for step in range(2, K + 1):
        mark(f'rs{step}')
        rs_step(step, lambda: None)
        if step < K:
            mark(f'own{step + 1}')
            own_parts(step + 1)
            each(done, done + 1, grads)
            done += 1
    def far_home():
        mark('farhome')
        settle(e_r.at[:, pl.ds(0, CAP)], e_recv)
        fw_s[...] = dot(sel_v[...], filled(e_r[...])).astype(BF)
        cp_fw.start()

    cp_fw = remote(fw_s, fw_r, fw_send, fw_recv, ydev_x(H))

    flatten_terms()
    mark('rsfinal')
    BPS = SUB // CAP

    def ret(peer, slot):
        used = pl.ds(0, CAP)
        return remote(ret_s.at[peer, used], ret_r.at[slot, used], ret_send, ret_recv, home(peer))

    for p in range(NS):
        mark(f'final{p}')
        ds = sub_ds[p]
        val = own_v[ds, :]
        for w in (0, 1):
            rs(w, K, p).wait_recv()
            val = val + rs_r[w * K + K - 1, ds, :].astype(F32)
        first_block = sub_ids[p] * BPS
        spread_rows = cmp_v[ds, pl.ds(pl.multiple_of(first_block * PC, 128), BPS * PC)]
        ret_s[pl.ds(first_block, BPS)] = dot(spread_rows, val.astype(BF), TN).astype(BF).reshape(BPS, PC, CW)

        def send_back(j, first_block=first_block):
            ret(first_block + j, ep).start()

        each(0, BPS, send_back)
        if p == 1:
            far_home()

    mark('gradsL')
    each(done, NY, grads)
    mark('rownorm')
    hb = D // CW

    def rowd(k):
        return remote(row_v.at[k], rowd_r, rd_send, rd_recv, partner)

    rowd(1 - c).start()

    rd_wait = rowd(1 - c)

    mark('router')
    settle(gf_r.at[pl.ds(0, TP - 1)], gf_recv)
    g_tot = gf_r[0]
    for j in range(1, TP):
        g_tot = g_tot + gf_r[j]
    g_tot = g_tot.astype(BF).astype(F32)
    d_w = dot((sel_v[...].astype(F32) * g_tot).astype(BF), one_hot(
        (iota((SLOTS, EP), 0) >> shift) == iota((SLOTS, EP), 1)))
    d_chosen = (d_w - jnp.sum(d_w * weights, axis=1, keepdims=True)) / total
    d_logits = (d_chosen * chosen * (1.0 - affinity) * hit32).astype(BF)
    zr_s[...] = dot(d_logits, tok_v[:, cols_x], TN)

    def zdev(off):
        return home(lax.rem(zc + off, NZ) * NX + xc)

    def zsend(d):
        return remote(zr_s, zr_r.at[zc], z_send, z_recv, zdev(d))

    each(0, NZ, lambda d: zsend(d).start())

    router_back = dot(d_logits, rw_v[:, cols_x])

    mark('rdwait')
    rd_wait.wait_recv()
    rowy_r[y] = (row_v[c] + rowd_r[...]).reshape(hb, CW).astype(BF)

    def ry(d):
        return remote(rowy_r.at[y], rowy_r.at[y], ry_send, ry_recv, ydev(d))

    each(1, NY, lambda d: ry(d).start())

    mark('retwait')
    settle(ret_r.at[:, pl.ds(0, CAP)], ret_recv)
    mark('combine')
    back = dot(sel_v[...], filled(ret_r[...]))
    cp_fw.wait_recv()
    tg_r[y, other] = (back + fw_r[...].astype(F32) + router_back).astype(BF)

    def tg(d):
        blk = tg_r.at[y, other]
        return remote(blk, blk, t_send, t_recv.at[y], ydev_x(d))

    def tg_wait(d):
        blk = tg_r.at[at(d), c]
        remote(blk, blk, t_send, t_recv.at[at(d)], ydev_x(d)).wait_recv()

    def tgd(src, core):
        blk = tg_r.at[src, core]
        return remote(blk, blk, td_send, td_recv, partner)

    each(0, NY - 1, lambda k: tg(y_order(k)).start())
    tgd(y, other).start()

    mark('zwait')
    settle(zr_r, z_recv)
    z_tot = zr_r[0]
    for j in range(1, NZ):
        z_tot = z_tot + zr_r[j]
    xr_r[xc] = z_tot

    def xdev(off):
        return {"ep": zc * NX + lax.rem(xc + off, NX)}

    def xsend(d):
        return remote(xr_r.at[xc], xr_r.at[xc], x_send, x_recv, xdev(d))

    each(1, NX, lambda d: xsend(d).start())
    mark('rywait')
    settle(rowy_r.at[pl.ds(0, NY - 1)], ry_recv)
    r_tot = rowy_r[0].astype(F32)
    for j in range(1, NY):
        r_tot = r_tot + rowy_r[j].astype(F32)
    rowf_s[c] = r_tot.reshape(hb, 1, CW)
    rf = remote(rowf_s.at[c], rowf_s.at[c], rf_send, rf_recv, partner)
    rf.start()
    mark('down')
    drow_o[...] = jnp.zeros_like(drow_o)
    each(0, NY, down_grads)
    mark('xwait')
    if NX > 1:
        settle(xr_r.at[pl.ds(0, NX - 1)], x_recv)
    x_tot = xr_r[0]
    for j in range(1, NX):
        x_tot = x_tot + xr_r[j]
    rg_o[...] = x_tot
    rr_o[...] = jnp.sum(x_tot * x_tot, axis=0, keepdims=True)

    mark('drain')
    for k in range(6):
        settle(a_s.at[k, :, pl.ds(0, CAP if k else PC)], a_send.at[k])
    settle(g_s, g_send)
    settle(ret_s.at[:, pl.ds(0, CAP)], ret_send)
    settle(gf_r.at[pl.ds(0, TP - 1)], gf_send)
    settle(zr_r, z_send)
    if NX > 1:
        settle(xr_r.at[pl.ds(0, NX - 1)], x_send)
    settle(rowy_r.at[pl.ds(0, NY - 1)], ry_send)
    settle(xa, d_send)
    settle(xa.at[pl.ds(0, 2 * H - 3)], y_send)
    settle(rs_s, rs_send)
    settle(e_s.at[:, pl.ds(0, CAP)], e_send)
    cp_fw.wait_send()
    cp_w.wait_send()
    for h in (0, 1):
        cp_gp(h).wait_send()
    rd_wait.wait_send()
    remote(rowf_s.at[1 - c], rowf_s.at[1 - c], rf_send, rf_recv, partner).wait_recv()
    rf.wait_send()

    mark('agwait')

    def arrive(k):
        d = y_order(NY - 2 - k)
        tg_wait(d)
        tgd(at(d), c).start()

    each(0, NY - 1, arrive)
    mark('agd')
    settle(tg_r.at[pl.ds(0, NY - 1), c], t_send)
    settle(tg_r.at[:, 1 - c], td_recv)
    settle(tg_r.at[:, c], td_send)
    mark(None)


def place(ny, tg, rg, rr, gg, ug, dg, rows, drow, tg_o, rg_o, rr_o, gg_o, ug_o, dg_o, gr_o, ur_o, drow_o, sem):
    pairs = [(gg, gg_o.at[0]), (ug, ug_o.at[0]), (dg, dg_o.at[0]), (rg, rg_o), (rr, rr_o),
             (rows.at[0], gr_o), (rows.at[1], ur_o), (drow, drow_o)]
    for j in range(ny):
        for k in (0, 1):
            pairs.append((tg.at[j, k], tg_o.at[:, pl.ds((2 * j + k) * CW, CW)]))
    copies = [pltpu.make_async_copy(a, b, sem.at[i]) for i, (a, b) in enumerate(pairs)]
    for cp in copies:
        cp.start()
    for cp in copies:
        cp.wait()


def build(ep, nx, ny, tok, width, cap):
    pc = 1
    while pc <= cap:
        pc *= 2
    rows, slots, tp, half = ep * cap, ep * pc, 2 * ny, ny // 2
    ns = rows // SUB
    hb = width // CW
    nz = ep // nx
    cfg = (ep, nx, ny, tok, width, cap, pc)
    v = pltpu.VMEM
    dma = pltpu.SemaphoreType.DMA
    scratch = [
        v((2, tok), jnp.int32), v((ep, width), BF),
        v((tok, width), BF), v((tok, width), BF), v((2, width, CW), BF), v((2, width, CW), BF), v((CW, width), BF),
        v((tok, slots), BF), v((rows, slots), BF),
        v((6, ep, pc, CW), BF), v((6, ep, pc, CW), BF),
        v((ny, 2, rows, CW), BF), v((ny, 2, rows, CW), BF),
        v((rows, CW), F32), v((rows, 2 * CW), F32), v((rows, CW), F32),
        v((rows, CW), BF), v((rows, 2 * CW), BF), v((rows, 2 * CW), BF), v((rows, CW), F32),
        v((rows, 2 * CW), F32), v((rows, CW), F32), v((2 * half - 2, rows, CW), BF), v((2 * half - 2, rows, CW), BF),
        v((ep, pc, CW), BF), v((ep, pc, CW), BF),
        v((ep, 1, CW), F32), v((ep, 1, CW), F32), v((tp, 1, slots), F32),
        v((ep, CW), F32), v((nz, ep, CW), F32), v((nx, ep, CW), F32),
        v((2, hb, 1, CW), F32), v((hb, 1, CW), F32), v((ny, hb, CW), BF),
        v((ep, pc, CW), BF), v((ep, pc, CW), BF), v((tok, CW), BF), v((tok, CW), BF),
        dma((7,)), dma((6,)), dma((6,)), dma, dma((2, half, 2)), dma, dma((2, ny)), dma, dma, dma((2,)), dma((2,)),
        dma, dma, dma, dma, dma, dma((2, half - 1, ns)), dma, dma, dma, dma, dma, dma, dma, dma, dma, dma, dma, dma,
        dma, dma((ny,)), dma, dma, dma, dma, dma, dma,
    ]
    sds = jax.ShapeDtypeStruct
    out_shape = (
        sds((ny, 2, tok, CW), BF), sds((ep, CW), F32), sds((1, CW), F32),
        sds((width, CW), BF), sds((width, CW), BF), sds((CW, width), BF),
        sds((2, hb, 1, CW), F32), sds((1, CW), F32),
    )
    vm = pl.BlockSpec(memory_space=pltpu.VMEM)
    hbm = pl.BlockSpec(memory_space=pltpu.HBM)
    anywhere = pl.BlockSpec(memory_space=pl.ANY)
    call = pl.pallas_call(
        functools.partial(kernel, cfg),
        out_shape=out_shape,
        in_specs=[hbm] * 7,
        out_specs=tuple([vm] * 8),
        scratch_shapes=scratch,
        compiler_params=pltpu.CompilerParams(
            collective_id=0, has_side_effects=True, vmem_limit_bytes=VMEM_MB * 1024 * 1024
        ),
        name="experts_backward",
    )
    finish = pl.pallas_call(
        functools.partial(place, ny),
        out_shape=(
            sds((tok, width), BF), sds((ep, CW), F32), sds((1, CW), F32),
            sds((1, width, CW), BF), sds((1, width, CW), BF), sds((1, CW, width), BF),
            sds((hb, 1, CW), F32), sds((hb, 1, CW), F32), sds((1, CW), F32),
        ),
        in_specs=[anywhere] * 8,
        out_specs=tuple([hbm] * 9),
        scratch_shapes=[dma((2 * ny + 8,))],
        compiler_params=pltpu.CompilerParams(vmem_limit_bytes=1024 * 1024),
        name="place_outputs",
    )

    def per_device(tokens, routing, router_weight, gate_weight, up_weight, down_weight, cotangent):
        args = (routing.T, router_weight.T, tokens, cotangent, gate_weight, up_weight, down_weight)
        parts = call(*[pltpu.with_memory_space_constraint(a, pltpu.HBM) for a in args])
        tg, rg, rr, gg, ug, dg, gr, ur, drow = finish(*parts)
        return (
            tg, rg.T, rr.reshape(CW), gg, ug, dg, gr.reshape(1, width), ur.reshape(1, width), drow,
        )

    return per_device


SPECS_IN = (
    P("ep", None), P("ep", None), P(), P("ep", None, "tp"), P("ep", None, "tp"), P("ep", "tp", None), P("ep", None),
)
SPECS_OUT = (
    P("ep", None), P("tp", None), P("tp"), P("ep", None, "tp"), P("ep", None, "tp"), P("ep", "tp", None),
    P("ep", None), P("ep", None), P("ep", "tp"),
)


def solution(mesh):
    ep, tp = mesh.shape["ep"], mesh.shape["tp"]
    body = build(ep, 4, tp // 2, 128, CW * tp, 14)
    return jax.shard_map(body, mesh=mesh, in_specs=SPECS_IN, out_specs=SPECS_OUT, check_vma=False)
```

```python
import functools

import jax
import jax.numpy as jnp
from jax import lax
from jax.experimental import pallas as pl
from jax.experimental.pallas import tpu as pltpu
from jax.sharding import PartitionSpec as P

BF = jnp.bfloat16
F32 = jnp.float32
CW = 128
VMEM_MB = 24
NN = ((1,), (0,))
NT = ((1,), (1,))
TN = ((0,), (0,))


def dot(a, b, dims=NN):
    return lax.dot_general(a, b, (dims, ((), ())), preferred_element_type=F32)


def iota(shape, dim):
    return lax.broadcasted_iota(jnp.int32, shape, dim)


def one_hot(mask, dtype=BF):
    return jnp.where(mask, 1.0, 0.0).astype(dtype)


def kernel(
    cfg,
    rt_h, rw_h, tok_h, cot_h, gw_h, uw_h, dw_h,
    tg_r, rg_o, rr_o, gg_o, ug_o, dg_o, rowf_s, drow_o,
    rt_v, rw_v, tok_v, cot_v, w_own, w_par, dn_v,
    sel_v, cmp_v, a_s, a_r, xa, za, wcol, acc_gu, acc_b,
    hid_v, gp_own, gp_par, tm_v, part_v, own_v, rs_s, rs_r, ret_s, ret_r,
    g_s, g_r, gf_r, zr_s, zr_r, xr_r, row_v, rowd_r, rowy_r, e_s, e_r, fw_s, fw_r,
    ld_sem, a_send, a_recv, y_send, y_recv, d_send, d_recv, w_send, w_recv, gp_send, gp_recv,
    g_send, g_recv, gf_send, gf_recv, rs_send, rs_recv, ret_send, ret_recv,
    z_send, z_recv, x_send, x_recv, rd_send, rd_recv, ry_send, ry_recv, rf_send, rf_recv,
    t_send, t_recv, td_send, td_recv, e_send, e_recv, fw_send, fw_recv,
):
    EP, NX, NY, T, D, CAP, PC = cfg
    cur = [None]

    def mark(n):
        if cur[0] is not None:
            cur[0].__exit__(None, None, None)
        cur[0] = None
        if n:
            cur[0] = jax.named_scope(n)
            cur[0].__enter__()

    NZ = EP // NX
    TP = 2 * NY
    H = NY // 2
    ROWS = EP * CAP
    SLOTS = EP * PC
    NS = min(4, NZ)
    WK = 2
    SUB = ROWS // NS
    HR = ROWS // 2
    HB = EP // 2
    HS = SLOTS // 2
    R0 = max(NZ // 4 - 1, 0)
    shift = PC.bit_length() - 1
    inv = 65536 // CAP + 1
    ep = lax.axis_index("ep")
    tp = lax.axis_index("tp")
    y = lax.div(tp, 2)
    c = lax.rem(tp, 2)
    zc = lax.div(ep, NX)
    xc = lax.rem(ep, NX)
    other = 1 - c
    partner = {"tp": y * 2 + other}

    def ydev(off):
        return {"tp": lax.rem(y + off + NY, NY) * 2 + c}

    def ydev_x(off):
        return {"tp": lax.rem(y + off + NY, NY) * 2 + other}

    def home(peer):
        return {"ep": peer, "tp": y * 2 + other}

    def core_at(dist):
        return other if dist % 2 else c

    def remote(src, dst, ss, rs, dev):
        return pltpu.make_async_remote_copy(
            src_ref=src, dst_ref=dst, send_sem=ss, recv_sem=rs, device_id=dev,
            device_id_type=pl.DeviceIdType.MESH,
        )

    def each(lo, hi, body):
        def step(i, carry):
            body(i)
            return carry

        lax.fori_loop(lo, hi, step, 0)

    mark('load')
    barrier = pltpu.get_barrier_semaphore()

    xs_of = [lax.rem(xc + NX // 2 + (j + 1) // 2 * (1 - 2 * (j % 2)), NX) for j in range(NX)]

    def y_order(k):
        return H + lax.div(k + 1, 2) * (1 - 2 * lax.rem(k, 2))

    def each_peer(body):
        def plane(k):
            dz = NZ // 2 + lax.div(k + 1, 2) * (1 - 2 * lax.rem(k, 2))
            base = lax.rem(zc + dz, NZ) * NX
            for x in xs_of:
                body(base + x)

        each(0, NZ - 1, plane)
        for x in xs_of[:-1]:
            body(zc * NX + x)

    def settle(ref, sem):
        pltpu.make_async_copy(ref, ref, sem).wait()

    near, far_half = (0, NZ // 2), (NZ // 2, NZ)
    def to_experts(span, body):
        def plane(q):
            base = lax.rem(zc + R0 - q + NZ, NZ) * NX
            for x in range(NX):
                body(base + x, q * NX + xc)

        each(span[0], span[1], plane)

    def to_homes(span, body):
        def plane(q):
            base = lax.rem(zc + q - R0 + NZ, NZ) * NX
            for x in range(NX):
                body(base + x, q * NX + x)

        each(span[0], span[1], plane)

    def greet_ep(peer):
        pl.semaphore_signal(barrier, inc=1, device_id=home(peer), device_id_type=pl.DeviceIdType.MESH)

    def greet_x(peer):
        pl.semaphore_signal(barrier, inc=1, device_id={"ep": peer}, device_id_type=pl.DeviceIdType.MESH)

    def greet_tp(d):
        pl.semaphore_signal(barrier, inc=1, device_id={"tp": lax.rem(tp + d, TP)},
                            device_id_type=pl.DeviceIdType.MESH)

    each_peer(greet_ep)
    for x in xs_of[:-1]:
        greet_x(zc * NX + x)
    each(1, TP, greet_tp)
    ld_rt = pltpu.make_async_copy(rt_h, rt_v, ld_sem.at[5])
    ld_rw = pltpu.make_async_copy(rw_h, rw_v, ld_sem.at[6])
    ld_tok = pltpu.make_async_copy(tok_h, tok_v, ld_sem.at[0])
    ld_cot = pltpu.make_async_copy(cot_h, cot_v, ld_sem.at[1])
    ld_g = pltpu.make_async_copy(gw_h.at[0], w_own.at[0], ld_sem.at[2])
    ld_u = pltpu.make_async_copy(uw_h.at[0], w_own.at[1], ld_sem.at[3])
    ld_d = pltpu.make_async_copy(dw_h.at[0], dn_v, ld_sem.at[4])
    for cp in (ld_rt, ld_tok, ld_rw, ld_cot, ld_g, ld_u, ld_d):
        cp.start()

    mark('tables')
    ld_rt.wait()
    e_row = iota((EP, T), 0)
    hit_t = one_hot((e_row == rt_v[0:1, :]) | (e_row == rt_v[1:2, :]))
    hit = dot(hit_t, one_hot(iota((EP, EP), 0) == iota((EP, EP), 1)), TN).astype(BF)
    earlier = one_hot(iota((T, T), 1) < iota((T, T), 0))
    count = dot(earlier, hit).astype(BF)
    spread = one_hot((iota((EP, SLOTS), 1) >> shift) == iota((EP, SLOTS), 0))
    slot_lane = (iota((T, SLOTS), 1) & (PC - 1)).astype(F32)
    sel = jnp.where((dot(count, spread) == slot_lane) & (dot(hit, spread) > 0.5), 1.0, 0.0)
    sel_v[...] = sel.astype(BF)
    lane_of = one_hot((iota((SLOTS, CW), 0) & (PC - 1)) == iota((SLOTS, CW), 1))
    tail = one_hot(
        ((iota((SLOTS, EP), 0) >> shift) == iota((SLOTS, EP), 1))
        & ((iota((SLOTS, EP), 0) & (PC - 1)) == CAP)
    )
    row_id = iota((ROWS, SLOTS), 0)
    row_src = (row_id * inv) >> 16
    cmp_v[...] = one_hot(iota((ROWS, SLOTS), 1) == row_id + (PC - CAP) * row_src)

    ld_tok.wait()
    ld_rw.wait()
    affinity = jax.nn.sigmoid(dot(tok_v[...], rw_v[...], NT))
    hit32 = hit.astype(F32)
    chosen = affinity * hit32
    total = jnp.sum(chosen, axis=1, keepdims=True)
    weights = chosen / total
    wx = dot(weights.astype(BF), spread)
    slot_w = jnp.sum(sel * wx, axis=0, keepdims=True)
    w_rows = dot((spread.astype(F32) * slot_w).astype(BF), lane_of)
    sel_b = sel.astype(BF)

    def at(off):
        return lax.rem(y + off + NY, NY)

    def col_ds(chip):
        return pl.ds(pl.multiple_of((chip * 2 + other) * CW, CW), CW)

    cols_x = col_ds(y)
    extra = ((0, y), (1, y), (0, at(H)), (1, at(H)), (1, at(H - 1)), (1, at(1 - H)))
    ld_cot.wait()

    def fill(k):
        kind, chip = extra[k]
        val = dot(sel_b, (tok_v if kind == 0 else cot_v)[:, col_ds(chip)], TN)
        if k == WK:
            val = val + dot(tail, w_rows.astype(BF))
        a_s[k] = val.astype(BF).reshape(EP, PC, CW)

    for k in range(6):
        fill(k)
    mark('barrier')
    pl.semaphore_wait(barrier, EP - 1 + NX - 1 + TP - 1)

    mark('a2a_issue')

    def a2a(k, h, peer, slot):
        used = pl.ds(0, PC if k == WK else CAP)
        return remote(a_s.at[k, peer, used], a_r.at[k, slot, used], a_send.at[k], a_recv.at[k, h], home(peer))

    def dot_exact(picks, vals, dims=NN, swap=False):
        hi = vals.astype(BF)
        lo = (vals - hi.astype(F32)).astype(BF)
        if swap:
            return dot(hi, picks, dims) + dot(lo, picks, dims)
        return dot(picks, hi, dims) + dot(picks, lo, dims)

    def filled(tiles):
        return jnp.where(iota(tiles.shape, 1) < CAP, tiles, jnp.zeros_like(tiles)).reshape(-1, CW)

    for k in range(6):
        for h, span in ((0, near), (1, far_half)) if k < 2 else ((1, far_half), (0, near)):
            to_experts(span, lambda p, slot, k=k, h=h: a2a(k, h, p, slot).start())
    ld_g.wait()
    ld_u.wait()
    ld_d.wait()
    cp_w = remote(w_own, w_par, w_send, w_recv, partner)
    cp_w.start()

    bufs = (xa, za)

    def half_of(part, src, core, h):
        return bufs[part].at[src, core, pl.ds(h * HR, HR)]

    def hop(way, step, part, h, src, sending=True):
        blk = half_of(part, src, core_at(step - 1 if sending else step), h)
        return remote(blk, blk, y_send, y_recv.at[way, step - 1, part, h], ydev_x(1 if way == 0 else -1))

    def cross(part, src, core, h):
        blk = half_of(part, src, core, h)
        return remote(blk, blk, d_send, d_recv.at[part, src], partner)

    def cross_wait(part, src):
        blk = bufs[part].at[src, c]
        remote(blk, blk, d_send, d_recv.at[part, src], partner).wait_recv()

    def parts_of(way, step):
        return (0, 1) if step < H - 1 else (0,)

    def take(k, h):
        kind, chip = extra[k]
        blocks = pl.ds(h * HB, HB)
        settle(a_r.at[k, blocks, pl.ds(0, PC if k == WK else CAP)], a_recv.at[k, h])
        tiles = a_r[k, blocks].reshape(HS, CW) if k == WK else filled(a_r[k, blocks])
        bufs[kind][chip, c, h * HR:(h + 1) * HR] = dot(cmp_v[0:HR, 0:HS], tiles).astype(BF)
        cross(kind, chip, c, h).start()

    for k in (0, 1):
        for h in (0, 1):
            mark(f'a2a_wait{k}{h}')
            take(k, h)
            for way in (0, 1):
                if k in parts_of(way, 1):
                    hop(way, 1, k, h, y).start()
    acc_gu[...] = jnp.zeros_like(acc_gu)
    acc_b[...] = jnp.zeros_like(acc_b)

    def chunk_ds(src):
        return pl.ds(pl.multiple_of(src * 2 * CW, 2 * CW), 2 * CW)

    def forward_x(src):
        cross_wait(0, src)
        xs = jnp.concatenate([xa[src, 0], xa[src, 1]], axis=1)
        ds = chunk_ds(src)
        wgu = jnp.concatenate([w_own[0, ds, :], w_own[1, ds, :]], axis=1)
        acc_gu[...] += dot(xs, wgu)

    def forward_z(src):
        cross_wait(1, src)
        zs = jnp.concatenate([za[src, 0], za[src, 1]], axis=1)
        acc_b[...] += dot(zs, dn_v[:, chunk_ds(src)], NT)

    def forward_chunk(src):
        forward_x(src)
        forward_z(src)

    def receive(s, part):
        mark(f'gather{s}{part}')
        for h in (0, 1):
            for way in (0, 1):
                if part in parts_of(way, s):
                    src = at(-s if way == 0 else s)
                    hop(way, s, part, h, src, False).wait_recv()
                    if s < H - 1 and part in parts_of(way, s + 1):
                        hop(way, s + 1, part, h, src).start()
                    cross(part, src, core_at(s), h).start()
        mark(f'fwd{s}{part}')

    def both(s, body):
        each(0, 2, lambda i: body(at((2 * i - 1) * s)))

    def extra_part(k):
        mark(f'extra{k}')
        take(k, 0)
        take(k, 1)

    def slot_weights():
        mark('wcol')
        pick = one_hot(
            iota((ROWS, SLOTS), 1) == (row_src * PC + CAP)
        )
        w_sel = dot(pick, a_r[WK].reshape(SLOTS, CW))
        r2 = iota((ROWS, CW), 0)
        r2_pos = r2 - ((r2 * inv) >> 16) * CAP
        w_masked = jnp.where(r2_pos == iota((ROWS, CW), 1), w_sel, 0.0)
        wcol[...] = jnp.broadcast_to(jnp.sum(w_masked, axis=1, keepdims=True), (ROWS, CW))

    mark('fwd0')
    each(0, 1, lambda i: forward_chunk(at(i)))
    if H == 4:
        receive(1, 0)
        extra_part(2)
        slot_weights()
        receive(1, 1)
        both(1, forward_x)
        extra_part(3)
        receive(2, 0)
        both(1, forward_z)
        each(0, 1, lambda i: forward_chunk(at(H + i)))
        extra_part(4)
        receive(2, 1)
        both(2, forward_x)
        extra_part(5)
        both(2, forward_z)
        receive(3, 0)
        both(3, forward_z)
        both(3, forward_x)
    else:
        for k in range(2, 6):
            extra_part(k)
        slot_weights()
        each(0, 1, lambda i: forward_chunk(at(H + i)))
        for s in range(1, H):
            for part in (0, 1) if s < H - 1 else (0,):
                receive(s, part)
            both(s, forward_x)
            both(s, forward_z)

    mark('pointwise')
    RB = 32 if ROWS % 64 == 0 and (ROWS // 2) % 32 == 0 else 16

    def pointwise(i):
        ds = pl.ds(pl.multiple_of(i * RB, RB), RB)
        pg = acc_gu[ds, :CW]
        pu = acc_gu[ds, CW:]
        bk = acc_b[ds, :]
        s = jax.nn.sigmoid(pg)
        hid = (pg * s * pu).astype(BF)
        hid_v[ds, :] = hid
        term = jnp.sum(hid.astype(F32) * bk, axis=1, keepdims=True)
        rr = iota((RB, CW), 0) + i * RB
        pos = rr - ((rr * inv) >> 16) * CAP
        tm_v[ds, :] = jnp.where(pos == iota((RB, CW), 1), term, 0.0)
        sc = wcol[ds, :] * bk
        gp_own[ds, :CW] = (sc * pu * s * (1.0 + pg * (1.0 - s))).astype(BF)
        gp_own[ds, CW:] = (sc * pg * s).astype(BF)

    def cp_gp(h):
        ds = pl.ds(h * HR, HR)
        return remote(gp_own.at[ds], gp_par.at[ds], gp_send.at[h], gp_recv.at[h], partner)

    for h in (1, 0):
        lax.fori_loop(h * (HR // RB), (h + 1) * (HR // RB), lambda i, carry: (pointwise(i), carry)[1], 0, unroll=True)
        cp_gp(h).start()

    mark('gpwait')
    def weight_rows(w_v, off, core):
        ds = pl.ds(pl.multiple_of(at(off) * 2 * CW + core * CW, CW), CW)
        return jnp.concatenate([w_v[0, ds, :], w_v[1, ds, :]], axis=1)

    K = H - 1

    def pair_parts(off_a, off_b, core_a, core_b, own_only=False, rows=slice(None), prior=None):
        def side(w_v):
            return jnp.concatenate([weight_rows(w_v, off_a, core_a), weight_rows(w_v, off_b, core_b)], axis=0)

        first = dot(gp_own[rows, :], side(w_own), NT) if prior is None else prior
        return first if own_only else first + dot(gp_par[rows, :], side(w_par), NT)

    sub_ids = [NS // 2] + list(range(NS // 2 + 1, NS)) + list(range(NS // 2 - 1, -1, -1))
    sub_ds = [pl.ds(i * SUB, SUB) for i in sub_ids]

    def rs(way, step, p):
        ds = sub_ds[p]
        return remote(rs_s.at[way * K + step - 1, ds], rs_r.at[way * K + step - 1, ds],
                      rs_send, rs_recv.at[way, step - 1, p],
                      ydev_x(1 if way == 0 else -1))

    own_first = pair_parts(K, -K, core_at(K), core_at(K), own_only=True)
    cp_w.wait_recv()
    for h in (1, 0):
        cp_gp(h).wait_recv()
        lo = h * HR
        pair = pair_parts(K, -K, core_at(K), core_at(K), rows=pl.ds(lo, HR), prior=own_first[lo:lo + HR]).astype(BF)
        for way in (0, 1):
            rs_s[way * K, pl.ds(lo, HR)] = pair[:, way * CW:(way + 1) * CW]
        for p in range(NS):
            if sub_ids[p] // (NS // 2) == h:
                for way in (0, 1):
                    rs(way, 1, p).start()

    def own_parts(step):
        part_v[...] = pair_parts(K - step + 1, step - K - 1, core_at(K - step + 1), core_at(K - step + 1))

    def rs_step(step, between):
        for i in range(NS):
            for w in (0, 1):
                ds = sub_ds[i]
                rs(w, step - 1, i).wait_recv()
                val = part_v[ds, w * CW:(w + 1) * CW] + rs_r[w * K + step - 2, ds, :].astype(F32)
                rs_s[w * K + step - 1, ds, :] = val.astype(BF)
                rs(w, step, i).start()
        between()

    mark('gterm')
    block_of = one_hot(((iota((EP, ROWS), 1) * inv) >> 16) == iota((EP, ROWS), 0))
    g_s[...] = dot_exact(block_of, tm_v[...]).reshape(EP, 1, CW)

    def g_copy(peer, slot):
        return remote(g_s.at[slot], g_r.at[ep], g_send, g_recv, home(peer))

    to_homes((0, NZ), lambda p, slot: g_copy(p, slot).start())

    ones = jnp.ones((8, 2 * CW), BF)

    def grads(src):
        ds = chunk_ds(src)
        xs = jnp.concatenate([xa[src, 0], xa[src, 1]], axis=1)
        gu = dot(xs, gp_own[...], TN)
        gg_o[ds, :] = gu[:, :CW].astype(BF)
        ug_o[ds, :] = gu[:, CW:].astype(BF)
        sq = (gu * gu).astype(BF)
        for k in (0, 1):
            tot = dot(ones[:, :CW], sq[:, k * CW:(k + 1) * CW], NT)
            row_v[k, pl.ds(src * 2, 1)] = tot[0:1, :CW].reshape(1, 1, CW)
            row_v[k, pl.ds(src * 2 + 1, 1)] = tot[0:1, CW:].reshape(1, 1, CW)

    def down_grads(src):
        ds = chunk_ds(src)
        scale = wcol[...]
        w0 = (scale * za[src, 0].astype(F32)).astype(BF)
        w1 = (scale * za[src, 1].astype(F32)).astype(BF)
        dgr = dot(hid_v[...], jnp.concatenate([w0, w1], axis=1), TN)
        dg_o[:, ds] = dgr.astype(BF)
        drow_o[...] += dot(ones, (dgr * dgr).astype(BF), NT)[0:1]

    def flatten_terms():
        mark('gflat')
        settle(g_r, g_recv)
        g_flat = jnp.sum(
            dot_exact(lane_of, g_r[...].reshape(EP, CW), NT, swap=True) * spread.astype(F32), axis=0, keepdims=True)
        gf_r[tp] = g_flat

        def gf(peer, slot):
            return remote(gf_r.at[tp], gf_r.at[slot], gf_send, gf_recv, {"tp": peer})

        def tpeer(d):
            return lax.rem(tp + d, TP)

        each(1, TP, lambda d: gf(tpeer(d), tp).start())

    mark('own2')
    if K > 1:
        own_parts(2)
    mark('far')
    far_near = pair_parts(H, 0, other, c)
    own_v[...] = far_near[:, CW:]
    e_s[...] = dot(cmp_v[...], far_near[:, :CW].astype(BF), TN).astype(BF).reshape(EP, PC, CW)

    def far(peer, slot):
        used = pl.ds(0, CAP)
        return remote(e_s.at[slot, used], e_r.at[ep, used], e_send, e_recv, home(peer))

    to_homes((0, NZ), lambda p, slot: far(p, slot).start())
    done = 0
    for step in range(2, K + 1):
        mark(f'rs{step}')
        rs_step(step, lambda: None)
        if step < K:
            mark(f'own{step + 1}')
            own_parts(step + 1)
    def far_home():
        mark('farhome')
        settle(e_r.at[:, pl.ds(0, CAP)], e_recv)
        fw_s[...] = dot(sel_v[...], filled(e_r[...])).astype(BF)
        cp_fw.start()

    cp_fw = remote(fw_s, fw_r, fw_send, fw_recv, ydev_x(H))

    flatten_terms()
    mark('rsfinal')
    BPS = SUB // CAP

    def ret(peer, slot):
        used = pl.ds(0, CAP)
        return remote(ret_s.at[slot, used], ret_r.at[ep, used], ret_send, ret_recv, home(peer))

    for p in range(NS):
        mark(f'final{p}')
        ds = sub_ds[p]
        val = own_v[ds, :]
        for w in (0, 1):
            rs(w, K, p).wait_recv()
            val = val + rs_r[w * K + K - 1, ds, :].astype(F32)
        first_block = sub_ids[p] * BPS
        ret_s[first_block:first_block + BPS] = dot(
            cmp_v[0:SUB, 0:BPS * PC], val.astype(BF), TN).astype(BF).reshape(BPS, PC, CW)
        planes = BPS // NX
        to_homes((sub_ids[p] * planes, (sub_ids[p] + 1) * planes), lambda b, slot: ret(b, slot).start())
        if p == 1:
            far_home()

    mark('gradsL')
    each(done, NY, grads)
    mark('rownorm')
    hb = D // CW

    def rowd(k):
        return remote(row_v.at[k], rowd_r, rd_send, rd_recv, partner)

    rowd(1 - c).start()

    rd_wait = rowd(1 - c)

    mark('router')
    settle(gf_r.at[pl.ds(0, TP - 1)], gf_recv)
    g_tot = gf_r[0]
    for j in range(1, TP):
        g_tot = g_tot + gf_r[j]
    g_tot = g_tot.astype(BF).astype(F32)
    d_w = dot((sel_v[...].astype(F32) * g_tot).astype(BF), one_hot(
        (iota((SLOTS, EP), 0) >> shift) == iota((SLOTS, EP), 1)))
    d_chosen = (d_w - jnp.sum(d_w * weights, axis=1, keepdims=True)) / total
    d_logits = (d_chosen * chosen * (1.0 - affinity) * hit32).astype(BF)
    zr_s[...] = dot(d_logits, tok_v[:, cols_x], TN).astype(BF)

    def zdev(off):
        return home(lax.rem(zc + off, NZ) * NX + xc)

    def zsend(d):
        return remote(zr_s, zr_r.at[zc], z_send, z_recv, zdev(d))

    each(0, NZ, lambda d: zsend(d).start())

    router_back = dot(d_logits, rw_v[:, cols_x])

    mark('rdwait')
    rd_wait.wait_recv()
    rowy_r[y] = (row_v[c] + rowd_r[...]).reshape(hb, CW).astype(BF)

    def ry(d):
        return remote(rowy_r.at[y], rowy_r.at[y], ry_send, ry_recv, ydev(d))

    each(1, NY, lambda d: ry(d).start())

    mark('retwait')
    settle(ret_r.at[:, pl.ds(0, CAP)], ret_recv)
    mark('combine')
    back = dot(sel_v[...], filled(ret_r[...]))
    cp_fw.wait_recv()
    tg_r[y, other] = (back + fw_r[...].astype(F32) + router_back).astype(BF)

    def tg(d):
        blk = tg_r.at[y, other]
        return remote(blk, blk, t_send, t_recv.at[y], ydev_x(d))

    def tg_wait(d):
        blk = tg_r.at[at(d), c]
        remote(blk, blk, t_send, t_recv.at[at(d)], ydev_x(d)).wait_recv()

    def tgd(src, core):
        blk = tg_r.at[src, core]
        return remote(blk, blk, td_send, td_recv, partner)

    each(0, NY - 1, lambda k: tg(y_order(k)).start())
    tgd(y, other).start()

    mark('down')
    drow_o[...] = jnp.zeros_like(drow_o)
    each(0, NY, down_grads)
    mark('zwait')
    settle(zr_r, z_recv)
    z_tot = zr_r[0].astype(F32)
    for j in range(1, NZ):
        z_tot = z_tot + zr_r[j].astype(F32)
    xr_r[xc] = z_tot

    def xdev(off):
        return {"ep": zc * NX + lax.rem(xc + off, NX)}

    def xsend(d):
        return remote(xr_r.at[xc], xr_r.at[xc], x_send, x_recv, xdev(d))

    each(1, NX, lambda d: xsend(d).start())
    mark('rywait')
    settle(rowy_r.at[pl.ds(0, NY - 1)], ry_recv)
    r_tot = rowy_r[0].astype(F32)
    for j in range(1, NY):
        r_tot = r_tot + rowy_r[j].astype(F32)
    rowf_s[c] = r_tot.reshape(hb, 1, CW)
    rf = remote(rowf_s.at[c], rowf_s.at[c], rf_send, rf_recv, partner)
    rf.start()
    mark('drain')
    for k in range(6):
        settle(a_s.at[k, :, pl.ds(0, PC if k == WK else CAP)], a_send.at[k])
    settle(g_s, g_send)
    settle(ret_s.at[:, pl.ds(0, CAP)], ret_send)
    settle(gf_r.at[pl.ds(0, TP - 1)], gf_send)
    settle(zr_r, z_send)
    settle(rowy_r.at[pl.ds(0, NY - 1)], ry_send)
    settle(xa, d_send)
    settle(xa.at[pl.ds(0, 2 * H - 3)], y_send)
    settle(rs_s, rs_send)
    settle(e_s.at[:, pl.ds(0, CAP)], e_send)
    cp_fw.wait_send()
    cp_w.wait_send()
    for h in (0, 1):
        cp_gp(h).wait_send()
    rd_wait.wait_send()

    mark('agwait')

    def arrive(k):
        d = y_order(NY - 2 - k)
        tg_wait(d)
        tgd(at(d), c).start()

    each(0, NY - 1, arrive)
    mark('xwait')
    if NX > 1:
        settle(xr_r.at[pl.ds(0, NX - 1)], x_recv)
    x_tot = xr_r[0]
    for j in range(1, NX):
        x_tot = x_tot + xr_r[j]
    rg_o[...] = x_tot
    rr_o[...] = jnp.sum(x_tot * x_tot, axis=0, keepdims=True)

    mark('agd')
    if NX > 1:
        settle(xr_r.at[pl.ds(0, NX - 1)], x_send)
    remote(rowf_s.at[1 - c], rowf_s.at[1 - c], rf_send, rf_recv, partner).wait_recv()
    rf.wait_send()
    settle(tg_r.at[pl.ds(0, NY - 1), c], t_send)
    settle(tg_r.at[:, 1 - c], td_recv)
    settle(tg_r.at[:, c], td_send)
    mark(None)


def place(ny, tg, rg, rr, gg, ug, dg, rows, drow, tg_o, rg_o, rr_o, gg_o, ug_o, dg_o, gr_o, ur_o, drow_o, sem):
    pairs = [(gg, gg_o.at[0]), (ug, ug_o.at[0]), (dg, dg_o.at[0]), (rg, rg_o), (rr, rr_o),
             (rows.at[0], gr_o), (rows.at[1], ur_o), (drow, drow_o)]
    for j in range(ny):
        for k in (0, 1):
            pairs.append((tg.at[j, k], tg_o.at[:, pl.ds((2 * j + k) * CW, CW)]))
    copies = [pltpu.make_async_copy(a, b, sem.at[i]) for i, (a, b) in enumerate(pairs)]
    for cp in copies:
        cp.start()
    for cp in copies:
        cp.wait()


def build(ep, nx, ny, tok, width, cap):
    pc = 1
    while pc <= cap:
        pc *= 2
    rows, slots, tp, half = ep * cap, ep * pc, 2 * ny, ny // 2
    ns = min(4, ep // nx)
    hb = width // CW
    nz = ep // nx
    cfg = (ep, nx, ny, tok, width, cap, pc)
    v = pltpu.VMEM
    dma = pltpu.SemaphoreType.DMA
    scratch = [
        v((2, tok), jnp.int32), v((ep, width), BF),
        v((tok, width), BF), v((tok, width), BF), v((2, width, CW), BF), v((2, width, CW), BF), v((CW, width), BF),
        v((tok, slots), BF), v((rows, slots), BF),
        v((6, ep, pc, CW), BF), v((6, ep, pc, CW), BF),
        v((ny, 2, rows, CW), BF), v((ny, 2, rows, CW), BF),
        v((rows, CW), F32), v((rows, 2 * CW), F32), v((rows, CW), F32),
        v((rows, CW), BF), v((rows, 2 * CW), BF), v((rows, 2 * CW), BF), v((rows, CW), F32),
        v((rows, 2 * CW), F32), v((rows, CW), F32), v((2 * half - 2, rows, CW), BF), v((2 * half - 2, rows, CW), BF),
        v((ep, pc, CW), BF), v((ep, pc, CW), BF),
        v((ep, 1, CW), F32), v((ep, 1, CW), F32), v((tp, 1, slots), F32),
        v((ep, CW), BF), v((nz, ep, CW), BF), v((nx, ep, CW), F32),
        v((2, hb, 1, CW), F32), v((hb, 1, CW), F32), v((ny, hb, CW), BF),
        v((ep, pc, CW), BF), v((ep, pc, CW), BF), v((tok, CW), BF), v((tok, CW), BF),
        dma((7,)), dma((6,)), dma((6, 2)), dma, dma((2, half - 1, 2, 2)), dma, dma((2, ny)), dma, dma, dma((2,)), dma((2,)),
        dma, dma, dma, dma, dma, dma((2, half - 1, ns)), dma, dma, dma, dma, dma, dma, dma, dma, dma, dma, dma, dma,
        dma, dma((ny,)), dma, dma, dma, dma, dma, dma,
    ]
    sds = jax.ShapeDtypeStruct
    out_shape = (
        sds((ny, 2, tok, CW), BF), sds((ep, CW), F32), sds((1, CW), F32),
        sds((width, CW), BF), sds((width, CW), BF), sds((CW, width), BF),
        sds((2, hb, 1, CW), F32), sds((1, CW), F32),
    )
    vm = pl.BlockSpec(memory_space=pltpu.VMEM)
    hbm = pl.BlockSpec(memory_space=pltpu.HBM)
    anywhere = pl.BlockSpec(memory_space=pl.ANY)
    call = pl.pallas_call(
        functools.partial(kernel, cfg),
        out_shape=out_shape,
        in_specs=[hbm] * 7,
        out_specs=tuple([vm] * 8),
        scratch_shapes=scratch,
        compiler_params=pltpu.CompilerParams(
            collective_id=0, has_side_effects=True, vmem_limit_bytes=VMEM_MB * 1024 * 1024
        ),
        name="experts_backward",
    )
    finish = pl.pallas_call(
        functools.partial(place, ny),
        out_shape=(
            sds((tok, width), BF), sds((ep, CW), F32), sds((1, CW), F32),
            sds((1, width, CW), BF), sds((1, width, CW), BF), sds((1, CW, width), BF),
            sds((hb, 1, CW), F32), sds((hb, 1, CW), F32), sds((1, CW), F32),
        ),
        in_specs=[anywhere] * 8,
        out_specs=tuple([hbm] * 9),
        scratch_shapes=[dma((2 * ny + 8,))],
        compiler_params=pltpu.CompilerParams(vmem_limit_bytes=1024 * 1024),
        name="place_outputs",
    )

    def per_device(tokens, routing, router_weight, gate_weight, up_weight, down_weight, cotangent):
        args = (routing.T, router_weight.T, tokens, cotangent, gate_weight, up_weight, down_weight)
        parts = call(*[pltpu.with_memory_space_constraint(a, pltpu.HBM) for a in args])
        tg, rg, rr, gg, ug, dg, gr, ur, drow = finish(*parts)
        return (
            tg, rg.T, rr.reshape(CW), gg, ug, dg, gr.reshape(1, width), ur.reshape(1, width), drow,
        )

    return per_device


SPECS_IN = (
    P("ep", None), P("ep", None), P(), P("ep", None, "tp"), P("ep", None, "tp"), P("ep", "tp", None), P("ep", None),
)
SPECS_OUT = (
    P("ep", None), P("tp", None), P("tp"), P("ep", None, "tp"), P("ep", None, "tp"), P("ep", "tp", None),
    P("ep", None), P("ep", None), P("ep", "tp"),
)


def solution(mesh):
    ep, tp = mesh.shape["ep"], mesh.shape["tp"]
    body = build(ep, 4, tp // 2, 128, CW * tp, 14)
    return jax.shard_map(body, mesh=mesh, in_specs=SPECS_IN, out_specs=SPECS_OUT, check_vma=False)
```

```python
import functools

import jax
import jax.numpy as jnp
from jax import lax
from jax.experimental import pallas as pl
from jax.experimental.pallas import tpu as pltpu
from jax.sharding import PartitionSpec as P

BF = jnp.bfloat16
F32 = jnp.float32
CW = 128
VMEM_MB = 24
NN = ((1,), (0,))
NT = ((1,), (1,))
TN = ((0,), (0,))


def dot(a, b, dims=NN):
    return lax.dot_general(a, b, (dims, ((), ())), preferred_element_type=F32)


def iota(shape, dim):
    return lax.broadcasted_iota(jnp.int32, shape, dim)


def one_hot(mask, dtype=BF):
    return jnp.where(mask, 1.0, 0.0).astype(dtype)


def kernel(
    cfg,
    rt_h, rw_h, tok_h, cot_h, gw_h, uw_h, dw_h,
    tg_r, rg_o, rr_o, gg_o, ug_o, dg_o, rowf_s, drow_o,
    rt_v, rw_v, tok_v, cot_v, w_own, w_par, dn_v,
    sel_v, cmp_v, a_s, a_r, xa, za, wcol, acc_gu, acc_b,
    hid_v, gp_own, gp_par, tm_v, part_v, own_v, rs_s, rs_r, ret_s, ret_r,
    g_s, g_r, gf_r, zr_s, zr_r, xr_r, row_v, rowd_r, rowy_r, e_s, e_r, fw_s, fw_r,
    ld_sem, a_send, a_recv, y_send, y_recv, d_send, d_recv, w_send, w_recv, gp_send, gp_recv,
    g_send, g_recv, gf_send, gf_recv, rs_send, rs_recv, ret_send, ret_recv,
    z_send, z_recv, x_send, x_recv, rd_send, rd_recv, ry_send, ry_recv, rf_send, rf_recv,
    t_send, t_recv, td_send, td_recv, e_send, e_recv, fw_send, fw_recv,
):
    EP, NX, NY, T, D, CAP, PC = cfg
    cur = [None]

    def mark(n):
        if cur[0] is not None:
            cur[0].__exit__(None, None, None)
        cur[0] = None
        if n:
            cur[0] = jax.named_scope(n)
            cur[0].__enter__()

    NZ = EP // NX
    TP = 2 * NY
    H = NY // 2
    ROWS = EP * CAP
    SLOTS = EP * PC
    NS = min(4, NZ)
    WK = 2
    SUB = ROWS // NS
    HR = ROWS // 2
    HB = EP // 2
    HS = SLOTS // 2
    R0 = max(NZ // 4 - 1, 0)
    shift = PC.bit_length() - 1
    inv = 65536 // CAP + 1
    ep = lax.axis_index("ep")
    tp = lax.axis_index("tp")
    y = lax.div(tp, 2)
    c = lax.rem(tp, 2)
    zc = lax.div(ep, NX)
    xc = lax.rem(ep, NX)
    other = 1 - c
    partner = {"tp": y * 2 + other}

    def ydev(off):
        return {"tp": lax.rem(y + off + NY, NY) * 2 + c}

    def ydev_x(off):
        return {"tp": lax.rem(y + off + NY, NY) * 2 + other}

    def home(peer):
        return {"ep": peer, "tp": y * 2 + other}

    def core_at(dist):
        return other if dist % 2 else c

    def remote(src, dst, ss, rs, dev):
        return pltpu.make_async_remote_copy(
            src_ref=src, dst_ref=dst, send_sem=ss, recv_sem=rs, device_id=dev,
            device_id_type=pl.DeviceIdType.MESH,
        )

    def each(lo, hi, body):
        def step(i, carry):
            body(i)
            return carry

        lax.fori_loop(lo, hi, step, 0)

    mark('load')
    barrier = pltpu.get_barrier_semaphore()

    xs_of = [lax.rem(xc + NX // 2 + (j + 1) // 2 * (1 - 2 * (j % 2)), NX) for j in range(NX)]

    def y_order(k):
        return H + lax.div(k + 1, 2) * (1 - 2 * lax.rem(k, 2))

    def each_peer(body):
        def plane(k):
            dz = NZ // 2 + lax.div(k + 1, 2) * (1 - 2 * lax.rem(k, 2))
            base = lax.rem(zc + dz, NZ) * NX
            for x in xs_of:
                body(base + x)

        each(0, NZ - 1, plane)
        for x in xs_of[:-1]:
            body(zc * NX + x)

    def settle(ref, sem):
        pltpu.make_async_copy(ref, ref, sem).wait()

    near, far_half = (0, NZ // 2), (NZ // 2, NZ)
    def to_experts(span, body):
        def plane(q):
            base = lax.rem(zc + R0 - q + NZ, NZ) * NX
            for x in xs_of:
                body(base + x, q * NX + xc)

        each(span[0], span[1], plane)

    def to_homes(span, body):
        def plane(q):
            base = lax.rem(zc + q - R0 + NZ, NZ) * NX
            for x in xs_of:
                body(base + x, q * NX + x)

        each(span[0], span[1], plane)

    def greet_ep(peer):
        pl.semaphore_signal(barrier, inc=1, device_id=home(peer), device_id_type=pl.DeviceIdType.MESH)

    def greet_x(peer):
        pl.semaphore_signal(barrier, inc=1, device_id={"ep": peer}, device_id_type=pl.DeviceIdType.MESH)

    def greet_tp(d):
        pl.semaphore_signal(barrier, inc=1, device_id={"tp": lax.rem(tp + d, TP)},
                            device_id_type=pl.DeviceIdType.MESH)

    each_peer(greet_ep)
    for x in xs_of[:-1]:
        greet_x(zc * NX + x)
    each(1, TP, greet_tp)
    ld_rt = pltpu.make_async_copy(rt_h, rt_v, ld_sem.at[5])
    ld_rw = pltpu.make_async_copy(rw_h, rw_v, ld_sem.at[6])
    ld_tok = pltpu.make_async_copy(tok_h, tok_v, ld_sem.at[0])
    ld_cot = pltpu.make_async_copy(cot_h, cot_v, ld_sem.at[1])
    ld_g = pltpu.make_async_copy(gw_h.at[0], w_own.at[0], ld_sem.at[2])
    ld_u = pltpu.make_async_copy(uw_h.at[0], w_own.at[1], ld_sem.at[3])
    ld_d = pltpu.make_async_copy(dw_h.at[0], dn_v, ld_sem.at[4])
    for cp in (ld_rt, ld_tok, ld_rw, ld_cot, ld_g, ld_u, ld_d):
        cp.start()

    mark('tables')
    ld_rt.wait()
    e_row = iota((EP, T), 0)
    hit_t = one_hot((e_row == rt_v[0:1, :]) | (e_row == rt_v[1:2, :]))
    hit = dot(hit_t, one_hot(iota((EP, EP), 0) == iota((EP, EP), 1)), TN).astype(BF)
    earlier = one_hot(iota((T, T), 1) < iota((T, T), 0))
    count = dot(earlier, hit).astype(BF)
    spread = one_hot((iota((EP, SLOTS), 1) >> shift) == iota((EP, SLOTS), 0))
    slot_lane = (iota((T, SLOTS), 1) & (PC - 1)).astype(F32)
    sel = jnp.where((dot(count, spread) == slot_lane) & (dot(hit, spread) > 0.5), 1.0, 0.0)
    sel_v[...] = sel.astype(BF)
    lane_of = one_hot((iota((SLOTS, CW), 0) & (PC - 1)) == iota((SLOTS, CW), 1))
    tail = one_hot(
        ((iota((SLOTS, EP), 0) >> shift) == iota((SLOTS, EP), 1))
        & ((iota((SLOTS, EP), 0) & (PC - 1)) == CAP)
    )
    row_id = iota((ROWS, SLOTS), 0)
    row_src = (row_id * inv) >> 16
    cmp_v[...] = one_hot(iota((ROWS, SLOTS), 1) == row_id + (PC - CAP) * row_src)

    ld_tok.wait()
    ld_rw.wait()
    affinity = jax.nn.sigmoid(dot(tok_v[...], rw_v[...], NT))
    hit32 = hit.astype(F32)
    chosen = affinity * hit32
    total = jnp.sum(chosen, axis=1, keepdims=True)
    weights = chosen / total
    wx = dot(weights.astype(BF), spread)
    slot_w = jnp.sum(sel * wx, axis=0, keepdims=True)
    w_rows = dot((spread.astype(F32) * slot_w).astype(BF), lane_of)
    sel_b = sel.astype(BF)

    def at(off):
        return lax.rem(y + off + NY, NY)

    def col_ds(chip):
        return pl.ds(pl.multiple_of((chip * 2 + other) * CW, CW), CW)

    cols_x = col_ds(y)
    extra = ((0, y), (1, y), (0, at(H)), (1, at(H)), (1, at(H - 1)), (1, at(1 - H)))
    ld_cot.wait()

    def fill(k):
        kind, chip = extra[k]
        val = dot(sel_b, (tok_v if kind == 0 else cot_v)[:, col_ds(chip)], TN)
        if k == WK:
            val = val + dot(tail, w_rows.astype(BF))
        a_s[k] = val.astype(BF).reshape(EP, PC, CW)

    for k in range(6):
        fill(k)
    mark('barrier')
    pl.semaphore_wait(barrier, EP - 1 + NX - 1 + TP - 1)

    mark('a2a_issue')

    def a2a(k, h, peer, slot):
        used = pl.ds(0, PC if k == WK else CAP)
        return remote(a_s.at[k, peer, used], a_r.at[k, slot, used], a_send.at[k], a_recv.at[k, h], home(peer))

    def dot_exact(picks, vals, dims=NN, swap=False):
        hi = vals.astype(BF)
        lo = (vals - hi.astype(F32)).astype(BF)
        if swap:
            return dot(hi, picks, dims) + dot(lo, picks, dims)
        return dot(picks, hi, dims) + dot(picks, lo, dims)

    def filled(tiles):
        return jnp.where(iota(tiles.shape, 1) < CAP, tiles, jnp.zeros_like(tiles)).reshape(-1, CW)

    for k in range(6):
        for h, span in ((0, near), (1, far_half)) if k < 2 else ((1, far_half), (0, near)):
            to_experts(span, lambda p, slot, k=k, h=h: a2a(k, h, p, slot).start())
    ld_g.wait()
    ld_u.wait()
    ld_d.wait()
    cp_w = remote(w_own, w_par, w_send, w_recv, partner)
    cp_w.start()

    bufs = (xa, za)

    def half_of(part, src, core, h):
        return bufs[part].at[src, core, pl.ds(h * HR, HR)]

    def hop(way, step, part, h, src, sending=True):
        blk = half_of(part, src, core_at(step - 1 if sending else step), h)
        return remote(blk, blk, y_send, y_recv.at[way, step - 1, part, h], ydev_x(1 if way == 0 else -1))

    def cross(part, src, core, h):
        blk = half_of(part, src, core, h)
        return remote(blk, blk, d_send, d_recv.at[part, src], partner)

    def cross_wait(part, src):
        blk = bufs[part].at[src, c]
        remote(blk, blk, d_send, d_recv.at[part, src], partner).wait_recv()

    def parts_of(way, step):
        return (0, 1) if step < H - 1 else (0,)

    def take(k, h):
        kind, chip = extra[k]
        blocks = pl.ds(h * HB, HB)
        settle(a_r.at[k, blocks, pl.ds(0, PC if k == WK else CAP)], a_recv.at[k, h])
        tiles = a_r[k, blocks].reshape(HS, CW) if k == WK else filled(a_r[k, blocks])
        bufs[kind][chip, c, h * HR:(h + 1) * HR] = dot(cmp_v[0:HR, 0:HS], tiles).astype(BF)
        cross(kind, chip, c, h).start()

    for k in (0, 1):
        for h in (0, 1):
            mark(f'a2a_wait{k}{h}')
            take(k, h)
            for way in (0, 1):
                if k in parts_of(way, 1):
                    hop(way, 1, k, h, y).start()
    acc_gu[...] = jnp.zeros_like(acc_gu)
    acc_b[...] = jnp.zeros_like(acc_b)

    def chunk_ds(src):
        return pl.ds(pl.multiple_of(src * 2 * CW, 2 * CW), 2 * CW)

    def forward_x(src):
        cross_wait(0, src)
        xs = jnp.concatenate([xa[src, 0], xa[src, 1]], axis=1)
        ds = chunk_ds(src)
        wgu = jnp.concatenate([w_own[0, ds, :], w_own[1, ds, :]], axis=1)
        acc_gu[...] += dot(xs, wgu)

    def forward_z(src):
        cross_wait(1, src)
        zs = jnp.concatenate([za[src, 0], za[src, 1]], axis=1)
        acc_b[...] += dot(zs, dn_v[:, chunk_ds(src)], NT)

    def forward_chunk(src):
        forward_x(src)
        forward_z(src)

    def receive(s, part):
        mark(f'gather{s}{part}')
        for h in (0, 1):
            for way in (0, 1):
                if part in parts_of(way, s):
                    src = at(-s if way == 0 else s)
                    hop(way, s, part, h, src, False).wait_recv()
                    if s < H - 1 and part in parts_of(way, s + 1):
                        hop(way, s + 1, part, h, src).start()
                    cross(part, src, core_at(s), h).start()
        mark(f'fwd{s}{part}')

    def both(s, body):
        each(0, 2, lambda i: body(at((2 * i - 1) * s)))

    def extra_part(k):
        mark(f'extra{k}')
        take(k, 0)
        take(k, 1)

    def slot_weights():
        mark('wcol')
        pick = one_hot(
            iota((ROWS, SLOTS), 1) == (row_src * PC + CAP)
        )
        w_sel = dot(pick, a_r[WK].reshape(SLOTS, CW))
        r2 = iota((ROWS, CW), 0)
        r2_pos = r2 - ((r2 * inv) >> 16) * CAP
        w_masked = jnp.where(r2_pos == iota((ROWS, CW), 1), w_sel, 0.0)
        wcol[...] = jnp.broadcast_to(jnp.sum(w_masked, axis=1, keepdims=True), (ROWS, CW))

    mark('fwd0')
    each(0, 1, lambda i: forward_chunk(at(i)))
    if H == 4:
        receive(1, 0)
        extra_part(2)
        slot_weights()
        receive(1, 1)
        both(1, forward_x)
        extra_part(3)
        receive(2, 0)
        both(1, forward_z)
        each(0, 1, lambda i: forward_chunk(at(H + i)))
        extra_part(4)
        receive(2, 1)
        both(2, forward_x)
        extra_part(5)
        both(2, forward_z)
        receive(3, 0)
        both(3, forward_z)
        both(3, forward_x)
    else:
        for k in range(2, 6):
            extra_part(k)
        slot_weights()
        each(0, 1, lambda i: forward_chunk(at(H + i)))
        for s in range(1, H):
            for part in (0, 1) if s < H - 1 else (0,):
                receive(s, part)
            both(s, forward_x)
            both(s, forward_z)

    mark('pointwise')
    RB = 32 if ROWS % 64 == 0 and (ROWS // 2) % 32 == 0 else 16

    def pointwise(i):
        ds = pl.ds(pl.multiple_of(i * RB, RB), RB)
        pg = acc_gu[ds, :CW]
        pu = acc_gu[ds, CW:]
        bk = acc_b[ds, :]
        s = jax.nn.sigmoid(pg)
        hid = (pg * s * pu).astype(BF)
        hid_v[ds, :] = hid
        term = jnp.sum(hid.astype(F32) * bk, axis=1, keepdims=True)
        rr = iota((RB, CW), 0) + i * RB
        pos = rr - ((rr * inv) >> 16) * CAP
        tm_v[ds, :] = jnp.where(pos == iota((RB, CW), 1), term, 0.0)
        sc = wcol[ds, :] * bk
        gp_own[ds, :CW] = (sc * pu * s * (1.0 + pg * (1.0 - s))).astype(BF)
        gp_own[ds, CW:] = (sc * pg * s).astype(BF)

    def cp_gp(h):
        ds = pl.ds(h * HR, HR)
        return remote(gp_own.at[ds], gp_par.at[ds], gp_send.at[h], gp_recv.at[h], partner)

    for h in (1, 0):
        lax.fori_loop(h * (HR // RB), (h + 1) * (HR // RB), lambda i, carry: (pointwise(i), carry)[1], 0, unroll=True)
        cp_gp(h).start()

    mark('gpwait')
    def weight_rows(w_v, off, core):
        ds = pl.ds(pl.multiple_of(at(off) * 2 * CW + core * CW, CW), CW)
        return jnp.concatenate([w_v[0, ds, :], w_v[1, ds, :]], axis=1)

    K = H - 1

    def pair_parts(off_a, off_b, core_a, core_b, own_only=False, rows=slice(None), prior=None):
        def side(w_v):
            return jnp.concatenate([weight_rows(w_v, off_a, core_a), weight_rows(w_v, off_b, core_b)], axis=0)

        first = dot(gp_own[rows, :], side(w_own), NT) if prior is None else prior
        return first if own_only else first + dot(gp_par[rows, :], side(w_par), NT)

    sub_ids = [NS // 2] + list(range(NS // 2 + 1, NS)) + list(range(NS // 2 - 1, -1, -1))
    sub_ds = [pl.ds(i * SUB, SUB) for i in sub_ids]

    def rs(way, step, p):
        ds = sub_ds[p]
        return remote(rs_s.at[way * K + step - 1, ds], rs_r.at[way * K + step - 1, ds],
                      rs_send, rs_recv.at[way, step - 1, p],
                      ydev_x(1 if way == 0 else -1))

    own_first = pair_parts(K, -K, core_at(K), core_at(K), own_only=True)
    cp_w.wait_recv()
    for h in (1, 0):
        cp_gp(h).wait_recv()
        lo = h * HR
        pair = pair_parts(K, -K, core_at(K), core_at(K), rows=pl.ds(lo, HR), prior=own_first[lo:lo + HR]).astype(BF)
        for way in (0, 1):
            rs_s[way * K, pl.ds(lo, HR)] = pair[:, way * CW:(way + 1) * CW]
        for p in range(NS):
            if sub_ids[p] // (NS // 2) == h:
                for way in (0, 1):
                    rs(way, 1, p).start()

    def own_parts(step):
        part_v[...] = pair_parts(K - step + 1, step - K - 1, core_at(K - step + 1), core_at(K - step + 1))

    def rs_step(step, between):
        for i in range(NS):
            for w in (0, 1):
                ds = sub_ds[i]
                rs(w, step - 1, i).wait_recv()
                val = part_v[ds, w * CW:(w + 1) * CW] + rs_r[w * K + step - 2, ds, :].astype(F32)
                rs_s[w * K + step - 1, ds, :] = val.astype(BF)
                rs(w, step, i).start()
        between()

    mark('gterm')
    block_of = one_hot(((iota((EP, ROWS), 1) * inv) >> 16) == iota((EP, ROWS), 0))
    g_s[...] = dot_exact(block_of, tm_v[...]).reshape(EP, 1, CW)

    def g_copy(peer, slot):
        return remote(g_s.at[slot], g_r.at[ep], g_send, g_recv, home(peer))

    to_homes((0, NZ), lambda p, slot: g_copy(p, slot).start())

    ones = jnp.ones((8, 2 * CW), BF)

    def grads(src):
        ds = chunk_ds(src)
        xs = jnp.concatenate([xa[src, 0], xa[src, 1]], axis=1)
        gu = dot(xs, gp_own[...], TN)
        gg_o[ds, :] = gu[:, :CW].astype(BF)
        ug_o[ds, :] = gu[:, CW:].astype(BF)
        sq = (gu * gu).astype(BF)
        for k in (0, 1):
            tot = dot(ones[:, :CW], sq[:, k * CW:(k + 1) * CW], NT)
            row_v[k, pl.ds(src * 2, 1)] = tot[0:1, :CW].reshape(1, 1, CW)
            row_v[k, pl.ds(src * 2 + 1, 1)] = tot[0:1, CW:].reshape(1, 1, CW)

    def down_grads(src):
        ds = chunk_ds(src)
        scale = wcol[...]
        w0 = (scale * za[src, 0].astype(F32)).astype(BF)
        w1 = (scale * za[src, 1].astype(F32)).astype(BF)
        dgr = dot(hid_v[...], jnp.concatenate([w0, w1], axis=1), TN)
        dg_o[:, ds] = dgr.astype(BF)
        drow_o[...] += dot(ones, (dgr * dgr).astype(BF), NT)[0:1]

    def flatten_terms():
        mark('gflat')
        settle(g_r, g_recv)
        g_flat = jnp.sum(
            dot_exact(lane_of, g_r[...].reshape(EP, CW), NT, swap=True) * spread.astype(F32), axis=0, keepdims=True)
        gf_r[tp] = g_flat

        def gf(peer, slot):
            return remote(gf_r.at[tp], gf_r.at[slot], gf_send, gf_recv, {"tp": peer})

        def tpeer(d):
            return lax.rem(tp + d, TP)

        each(1, TP, lambda d: gf(tpeer(d), tp).start())

    mark('own2')
    if K > 1:
        own_parts(2)
    mark('far')
    far_near = pair_parts(H, 0, other, c)
    own_v[...] = far_near[:, CW:]
    e_s[...] = dot(cmp_v[...], far_near[:, :CW].astype(BF), TN).astype(BF).reshape(EP, PC, CW)

    def far(peer, slot):
        used = pl.ds(0, CAP)
        return remote(e_s.at[slot, used], e_r.at[ep, used], e_send, e_recv, home(peer))

    to_homes((0, NZ), lambda p, slot: far(p, slot).start())
    each(0, 1, grads)
    done = 1
    for step in range(2, K + 1):
        mark(f'rs{step}')
        rs_step(step, lambda: None)
        if step < K:
            mark(f'own{step + 1}')
            own_parts(step + 1)
    def far_home():
        mark('farhome')
        settle(e_r.at[:, pl.ds(0, CAP)], e_recv)
        fw_s[...] = dot(sel_v[...], filled(e_r[...])).astype(BF)
        cp_fw.start()

    cp_fw = remote(fw_s, fw_r, fw_send, fw_recv, ydev_x(H))

    flatten_terms()
    mark('rsfinal')
    BPS = SUB // CAP

    def ret(peer, slot):
        used = pl.ds(0, CAP)
        return remote(ret_s.at[slot, used], ret_r.at[ep, used], ret_send, ret_recv, home(peer))

    for p in range(NS):
        mark(f'final{p}')
        ds = sub_ds[p]
        val = own_v[ds, :]
        for w in (0, 1):
            rs(w, K, p).wait_recv()
            val = val + rs_r[w * K + K - 1, ds, :].astype(F32)
        first_block = sub_ids[p] * BPS
        ret_s[first_block:first_block + BPS] = dot(
            cmp_v[0:SUB, 0:BPS * PC], val.astype(BF), TN).astype(BF).reshape(BPS, PC, CW)
        planes = BPS // NX
        to_homes((sub_ids[p] * planes, (sub_ids[p] + 1) * planes), lambda b, slot: ret(b, slot).start())
        if p == 1:
            far_home()

    mark('gradsL')
    each(done, NY, grads)
    mark('rownorm')
    hb = D // CW

    def rowd(k):
        return remote(row_v.at[k], rowd_r, rd_send, rd_recv, partner)

    rowd(1 - c).start()

    rd_wait = rowd(1 - c)

    mark('router')
    settle(gf_r.at[pl.ds(0, TP - 1)], gf_recv)
    g_tot = gf_r[0]
    for j in range(1, TP):
        g_tot = g_tot + gf_r[j]
    g_tot = g_tot.astype(BF).astype(F32)
    d_w = dot((sel_v[...].astype(F32) * g_tot).astype(BF), one_hot(
        (iota((SLOTS, EP), 0) >> shift) == iota((SLOTS, EP), 1)))
    d_chosen = (d_w - jnp.sum(d_w * weights, axis=1, keepdims=True)) / total
    d_logits = (d_chosen * chosen * (1.0 - affinity) * hit32).astype(BF)
    zr_s[...] = dot(d_logits, tok_v[:, cols_x], TN).astype(BF)

    def zdev(off):
        return home(lax.rem(zc + off, NZ) * NX + xc)

    def zsend(d):
        return remote(zr_s, zr_r.at[zc], z_send, z_recv, zdev(d))

    each(0, NZ, lambda d: zsend(d).start())

    router_back = dot(d_logits, rw_v[:, cols_x])

    mark('rdwait')
    rd_wait.wait_recv()
    rowy_r[y] = (row_v[c] + rowd_r[...]).reshape(hb, CW).astype(BF)

    def ry(d):
        return remote(rowy_r.at[y], rowy_r.at[y], ry_send, ry_recv, ydev(d))

    each(1, NY, lambda d: ry(d).start())

    mark('retwait')
    settle(ret_r.at[:, pl.ds(0, CAP)], ret_recv)
    mark('combine')
    back = dot(sel_v[...], filled(ret_r[...]))
    cp_fw.wait_recv()
    tg_r[y, other] = (back + fw_r[...].astype(F32) + router_back).astype(BF)

    def tg(d):
        blk = tg_r.at[y, other]
        return remote(blk, blk, t_send, t_recv.at[y], ydev_x(d))

    def tg_wait(d):
        blk = tg_r.at[at(d), c]
        remote(blk, blk, t_send, t_recv.at[at(d)], ydev_x(d)).wait_recv()

    def tgd(src, core):
        blk = tg_r.at[src, core]
        return remote(blk, blk, td_send, td_recv, partner)

    each(0, NY - 1, lambda k: tg(y_order(k)).start())
    tgd(y, other).start()

    mark('down')
    drow_o[...] = jnp.zeros_like(drow_o)
    each(0, NY, down_grads)
    mark('zwait')
    settle(zr_r, z_recv)
    z_tot = zr_r[0].astype(F32)
    for j in range(1, NZ):
        z_tot = z_tot + zr_r[j].astype(F32)
    xr_r[xc] = z_tot

    def xdev(off):
        return {"ep": zc * NX + lax.rem(xc + off, NX)}

    def xsend(d):
        return remote(xr_r.at[xc], xr_r.at[xc], x_send, x_recv, xdev(d))

    each(1, NX, lambda d: xsend(d).start())
    mark('rywait')
    settle(rowy_r.at[pl.ds(0, NY - 1)], ry_recv)
    r_tot = rowy_r[0].astype(F32)
    for j in range(1, NY):
        r_tot = r_tot + rowy_r[j].astype(F32)
    rowf_s[c] = r_tot.reshape(hb, 1, CW)
    rf = remote(rowf_s.at[c], rowf_s.at[c], rf_send, rf_recv, partner)
    rf.start()
    mark('drain')
    for k in range(6):
        settle(a_s.at[k, :, pl.ds(0, PC if k == WK else CAP)], a_send.at[k])
    settle(g_s, g_send)
    settle(ret_s.at[:, pl.ds(0, CAP)], ret_send)
    settle(gf_r.at[pl.ds(0, TP - 1)], gf_send)
    settle(zr_r, z_send)
    settle(rowy_r.at[pl.ds(0, NY - 1)], ry_send)
    settle(xa, d_send)
    settle(xa.at[pl.ds(0, 2 * H - 3)], y_send)
    settle(rs_s, rs_send)
    settle(e_s.at[:, pl.ds(0, CAP)], e_send)
    cp_fw.wait_send()
    cp_w.wait_send()
    for h in (0, 1):
        cp_gp(h).wait_send()
    rd_wait.wait_send()

    mark('agwait')

    def arrive(k):
        d = y_order(NY - 2 - k)
        tg_wait(d)
        tgd(at(d), c).start()

    each(0, NY - 1, arrive)
    mark('xwait')
    if NX > 1:
        settle(xr_r.at[pl.ds(0, NX - 1)], x_recv)
    x_tot = xr_r[0]
    for j in range(1, NX):
        x_tot = x_tot + xr_r[j]
    rg_o[...] = x_tot
    rr_o[...] = jnp.sum(x_tot * x_tot, axis=0, keepdims=True)

    mark('agd')
    if NX > 1:
        settle(xr_r.at[pl.ds(0, NX - 1)], x_send)
    remote(rowf_s.at[1 - c], rowf_s.at[1 - c], rf_send, rf_recv, partner).wait_recv()
    rf.wait_send()
    settle(tg_r.at[pl.ds(0, NY - 1), c], t_send)
    settle(tg_r.at[:, 1 - c], td_recv)
    settle(tg_r.at[:, c], td_send)
    mark(None)


def place(ny, tg, rg, rr, gg, ug, dg, rows, drow, tg_o, rg_o, rr_o, gg_o, ug_o, dg_o, gr_o, ur_o, drow_o, sem):
    pairs = [(gg, gg_o.at[0]), (ug, ug_o.at[0]), (dg, dg_o.at[0]), (rg, rg_o), (rr, rr_o),
             (rows.at[0], gr_o), (rows.at[1], ur_o), (drow, drow_o)]
    for j in range(ny):
        for k in (0, 1):
            pairs.append((tg.at[j, k], tg_o.at[:, pl.ds((2 * j + k) * CW, CW)]))
    copies = [pltpu.make_async_copy(a, b, sem.at[i]) for i, (a, b) in enumerate(pairs)]
    for cp in copies:
        cp.start()
    for cp in copies:
        cp.wait()


def build(ep, nx, ny, tok, width, cap):
    pc = 1
    while pc <= cap:
        pc *= 2
    rows, slots, tp, half = ep * cap, ep * pc, 2 * ny, ny // 2
    ns = min(4, ep // nx)
    hb = width // CW
    nz = ep // nx
    cfg = (ep, nx, ny, tok, width, cap, pc)
    v = pltpu.VMEM
    dma = pltpu.SemaphoreType.DMA
    scratch = [
        v((2, tok), jnp.int32), v((ep, width), BF),
        v((tok, width), BF), v((tok, width), BF), v((2, width, CW), BF), v((2, width, CW), BF), v((CW, width), BF),
        v((tok, slots), BF), v((rows, slots), BF),
        v((6, ep, pc, CW), BF), v((6, ep, pc, CW), BF),
        v((ny, 2, rows, CW), BF), v((ny, 2, rows, CW), BF),
        v((rows, CW), F32), v((rows, 2 * CW), F32), v((rows, CW), F32),
        v((rows, CW), BF), v((rows, 2 * CW), BF), v((rows, 2 * CW), BF), v((rows, CW), F32),
        v((rows, 2 * CW), F32), v((rows, CW), F32), v((2 * half - 2, rows, CW), BF), v((2 * half - 2, rows, CW), BF),
        v((ep, pc, CW), BF), v((ep, pc, CW), BF),
        v((ep, 1, CW), F32), v((ep, 1, CW), F32), v((tp, 1, slots), F32),
        v((ep, CW), BF), v((nz, ep, CW), BF), v((nx, ep, CW), F32),
        v((2, hb, 1, CW), F32), v((hb, 1, CW), F32), v((ny, hb, CW), BF),
        v((ep, pc, CW), BF), v((ep, pc, CW), BF), v((tok, CW), BF), v((tok, CW), BF),
        dma((7,)), dma((6,)), dma((6, 2)), dma, dma((2, half - 1, 2, 2)), dma, dma((2, ny)), dma, dma, dma((2,)), dma((2,)),
        dma, dma, dma, dma, dma, dma((2, half - 1, ns)), dma, dma, dma, dma, dma, dma, dma, dma, dma, dma, dma, dma,
        dma, dma((ny,)), dma, dma, dma, dma, dma, dma,
    ]
    sds = jax.ShapeDtypeStruct
    out_shape = (
        sds((ny, 2, tok, CW), BF), sds((ep, CW), F32), sds((1, CW), F32),
        sds((width, CW), BF), sds((width, CW), BF), sds((CW, width), BF),
        sds((2, hb, 1, CW), F32), sds((1, CW), F32),
    )
    vm = pl.BlockSpec(memory_space=pltpu.VMEM)
    hbm = pl.BlockSpec(memory_space=pltpu.HBM)
    anywhere = pl.BlockSpec(memory_space=pl.ANY)
    call = pl.pallas_call(
        functools.partial(kernel, cfg),
        out_shape=out_shape,
        in_specs=[hbm] * 7,
        out_specs=tuple([vm] * 8),
        scratch_shapes=scratch,
        compiler_params=pltpu.CompilerParams(
            collective_id=0, has_side_effects=True, vmem_limit_bytes=VMEM_MB * 1024 * 1024
        ),
        name="experts_backward",
    )
    finish = pl.pallas_call(
        functools.partial(place, ny),
        out_shape=(
            sds((tok, width), BF), sds((ep, CW), F32), sds((1, CW), F32),
            sds((1, width, CW), BF), sds((1, width, CW), BF), sds((1, CW, width), BF),
            sds((hb, 1, CW), F32), sds((hb, 1, CW), F32), sds((1, CW), F32),
        ),
        in_specs=[anywhere] * 8,
        out_specs=tuple([hbm] * 9),
        scratch_shapes=[dma((2 * ny + 8,))],
        compiler_params=pltpu.CompilerParams(vmem_limit_bytes=1024 * 1024),
        name="place_outputs",
    )

    def per_device(tokens, routing, router_weight, gate_weight, up_weight, down_weight, cotangent):
        args = (routing.T, router_weight.T, tokens, cotangent, gate_weight, up_weight, down_weight)
        parts = call(*[pltpu.with_memory_space_constraint(a, pltpu.HBM) for a in args])
        tg, rg, rr, gg, ug, dg, gr, ur, drow = finish(*parts)
        return (
            tg, rg.T, rr.reshape(CW), gg, ug, dg, gr.reshape(1, width), ur.reshape(1, width), drow,
        )

    return per_device


SPECS_IN = (
    P("ep", None), P("ep", None), P(), P("ep", None, "tp"), P("ep", None, "tp"), P("ep", "tp", None), P("ep", None),
)
SPECS_OUT = (
    P("ep", None), P("tp", None), P("tp"), P("ep", None, "tp"), P("ep", None, "tp"), P("ep", "tp", None),
    P("ep", None), P("ep", None), P("ep", "tp"),
)


def solution(mesh):
    ep, tp = mesh.shape["ep"], mesh.shape["tp"]
    body = build(ep, 4, tp // 2, 128, CW * tp, 14)
    return jax.shard_map(body, mesh=mesh, in_specs=SPECS_IN, out_specs=SPECS_OUT, check_vma=False)
```
